256 devices in a mesh: grp: 2 (over y), sp: 32 (over z, core), tp: 4 (over x).
Axes of the slice: x: 4, y: 2, z: 16, core: 2. Of those that a mesh axis runs over, the one named last changes fastest.
The devices are a block of a 4x16x16 slice.
Arguments:
- queries: bfloat16 [14336, 1024], P(('grp', 'sp'), 'tp'), parts along dimension 0, may hold values from -6 to 6
- head_key_rows: bfloat16 [14336, 1024], P(('grp', 'sp'), 'tp'), parts along dimension 0, may hold values from -6 to 6
- head_value_rows: bfloat16 [14336, 2048], P(('grp', 'sp'), 'tp'), parts along dimension 0, may hold values from -6 to 6
- input_gate_logit: float32 [16, 14336], P('tp', ('grp', 'sp')), parts along dimension 1, may hold values from -6 to 300
- forget_gate_preact: float32 [16, 14336], P('tp', ('grp', 'sp')), parts along dimension 1, may hold values from 0 to 14
- forget_log_offset: float32 [16, 14336], P('tp', ('grp', 'sp')), parts along dimension 1, may hold values from -0.7 to 0
- per_head_norm_gain: bfloat16 [2048], P('tp'), may hold values from 0.099609375 to 1.8984375
- cell_output_matrix: bfloat16 [2048, 2048], P('tp', 'sp'), may hold values from -0.125 to 0.125
- layer_input_rows: bfloat16 [14336, 2048], P(('grp', 'sp', 'tp')), parts along dimension 0, may hold values from -6 to 6
- expert_norm_gain: bfloat16 [2048], replicated, may hold values from 0.099609375 to 1.8984375
- chosen_expert_index: int32 [14336, 2], P(('grp', 'sp', 'tp')), parts along dimension 0, may hold values from 0 to 31, all different within a row; in each aligned block of 56 rows (0 to 55, 56 to 111, ...) at most 7 rows name the same one
- chosen_expert_weight: float32 [14336, 2], P(('grp', 'sp', 'tp')), parts along dimension 0, may hold values from 0.2 to 1
- expert_gate_matrix: bfloat16 [32, 2048, 3584], P('sp', None, 'tp'), may hold values from -0.125 to 0.125
- expert_up_matrix: bfloat16 [32, 2048, 3584], P('sp', None, 'tp'), may hold values from -0.125 to 0.125
- expert_down_matrix: bfloat16 [32, 3584, 2048], P('sp', 'tp'), may hold values from -0.09375 to 0.09375
Outputs:
- layer_out: bfloat16 [14336, 2048], P(('grp', 'sp', 'tp')), parts along dimension 0
The draws below stay inside these ranges and needn't reach their ends.
There are 2 independent parts, one for each index of `grp`. The reference program is written for one: setup_inputs(seed, part) draws one part's arguments, and reference() takes and returns one part's arrays. A program takes and returns all parts, laid end to end along the dimension named above; an argument that names none is the same for every part. Nothing has to cross between parts.
Inputs may be any that keep to these rules, and one draw needn't show every extreme that they name: `chosen_expert_index`: each row names 2 different experts. In the rows of one device no expert is named more than 7 times, and in every draw some expert is named exactly 7 times in the rows of some device.
All inputs are finite; a program needn't handle non-finite values.
Results may differ from the reference program's by a relative error of at most 0.013.
Values may be sent and summed in bfloat16 or wider, within the bound.
No kernel may reach another device: no remote copies, remote signals or barrier semaphores. Data moves between devices by JAX's collectives and lax.ppermute only.
A program may use at most 64 MiB of HBM per device.

```python
import math
import jax
import jax.numpy as jnp
import numpy as np
from jax import lax

D = 2048
HEADS = 16
DK = 64
DV = 128
FF = 3584
TOK_DEV = 224
TOKENS = 7168
ROWS_DEV = 56
EXPERTS = 32
SLOTS = 7
N_TP = 4


def draw_input_gate_logit(key, part):
    first = jax.random.fold_in(jax.random.fold_in(key, 11), 0)
    return jnp.clip(jax.random.normal(first, (HEADS, TOKENS), jnp.float32), -6.0, 6.0)


def draw_forget_gate_preact(key, part):
    first, second, third = jax.random.split(jax.random.fold_in(key, 23), 3)
    share = 0.5
    fast = jax.random.uniform(first, (HEADS, 1), jnp.float32) < share
    level = jnp.where(fast, math.log(40.0), math.log(TOKENS) + 1.0)
    blocks = TOKENS // TOK_DEV
    shift = jax.random.uniform(second, (HEADS, blocks, 1), jnp.float32, -0.7, 0.7)
    shift = jnp.broadcast_to(shift, (HEADS, blocks, TOK_DEV)).reshape(HEADS, TOKENS)
    noise = 0.7 * jnp.clip(jax.random.normal(third, (HEADS, TOKENS), jnp.float32), -3.0, 3.0)
    return level + shift + noise


def draw_forget_log_offset(key, part):
    first, second = jax.random.split(jax.random.fold_in(key, 37))
    spots = jax.random.uniform(first, (HEADS, TOKENS), jnp.float32) < 6.0 / TOKENS
    losses = jnp.log(jax.random.uniform(second, (HEADS, TOKENS), jnp.float32, 0.5, 0.8))
    return jnp.where(spots, losses, 0.0)


def steps_of(key, dims, cuts, least, high):
    factor_of = 1.0
    for dim, shards_of in cuts:
        draws = jax.random.uniform(jax.random.fold_in(jax.random.fold_in(key, 6), dim), (shards_of,), jnp.float32, least / len(cuts), high / len(cuts))
        factor_of = factor_of * jnp.repeat(jnp.exp(draws), dims[dim] // shards_of).reshape((-1,) + (1,) * (len(dims) - 1 - dim))
    return factor_of


def deal_out(stream_key, own, number, rows, count, top, most, slope):
    order = jax.random.permutation(stream_key, count)
    heavy_load, ordinary = shares(count, rows * top, most, slope, True), shares(count, rows * top, most, slope, False)
    places = jnp.arange(count)

    def named(tallies, offset_by):
        used = int((tallies > 0).sum())
        fixed = max(1, used // 4)
        passed = fixed + (places - fixed + offset_by * (used - fixed)) % max(1, count - fixed)
        return jnp.zeros((count,), jnp.int32).at[order[jnp.where(places < fixed, places, passed)]].set(jnp.asarray(tallies, jnp.int32))

    tallies = jnp.where(number % 4 == 0, named(heavy_load, number // 4), named(ordinary, number - number // 4 - 1))
    mixed = jax.random.permutation(jax.random.fold_in(own, 3), count)
    giver, taker = mixed[0:count // 2 * 2:2], mixed[1:count // 2 * 2:2]
    slack = jnp.minimum(tallies[giver] - 1, most - tallies[taker]) // 2
    slack = jnp.where((giver == order[0]) | (taker == order[0]) | (tallies[taker] == 0), 0, jnp.maximum(slack, 0))
    passed = jax.random.randint(jax.random.fold_in(own, 4), (count // 2,), 0, 1 << 20) % (slack + 1)
    tallies = tallies.at[giver].add(-passed).at[taker].add(passed)
    items = jnp.searchsorted(jnp.cumsum(tallies), jnp.arange(rows * top), side="right").astype(jnp.int32)
    grid = items.reshape(top, rows).T
    grid = grid[jax.random.permutation(jax.random.fold_in(own, 1), rows)]
    offset_by = jax.random.randint(jax.random.fold_in(own, 2), (rows, 1), 0, top)
    return jnp.take_along_axis(grid, (jnp.arange(top)[None, :] + offset_by) % top, axis=1)


def shares(count, total, bound, skew, full):
    portions = [(1 << 20) // math.isqrt(rank ** skew) + 1 for rank in range(1, count + 1)]
    largest = bound if full else min(bound, max(-(-total // count), total * portions[0] // sum(portions)))
    least = 1 if total - largest >= count - 1 else 0
    given, spare = [largest] + [least] * (count - 1), total - largest - least * (count - 1)
    while spare > 0:
        free = [i for i in range(1, count) if given[i] < largest] or [i for i in range(1, count) if given[i] < bound]
        whole, left = sum([portions[i] for i in free]), spare
        for i in free:
            extra = min(bound - given[i], max(1, left * portions[i] // whole), spare)
            given[i] = given[i] + extra
            spare = spare - extra
    return np.array(given)


def gaussian(key, dims, spread, reach, shards=(), kind=jnp.bfloat16):
    entries = jax.random.normal(key, dims, jnp.float32) * spread
    if len(shards) > 0:
        entries = steps_of(key, dims, shards, -0.22, 0.18) * entries
    return jnp.clip(entries, min=-reach, max=reach).astype(kind)


def setup_inputs(seed: int = 0, part: int = 0) -> dict:
    keys = jax.random.split(jax.random.key(seed), 16)
    own_keys = jax.random.split(jax.random.fold_in(keys[15], part), 16)
    queries = gaussian(own_keys[0], (TOKENS, HEADS * DK), 1.0, 6.0, ((0, 32), (1, 4)))
    head_key_rows = gaussian(own_keys[1], (TOKENS, HEADS * DK), 1.0, 6.0, ((0, 32), (1, 4)))
    head_value_rows = gaussian(own_keys[2], (TOKENS, HEADS * DV), 1.0, 6.0, ((0, 32), (1, 4)))
    input_gate_logit = draw_input_gate_logit(jax.random.fold_in(jax.random.fold_in(keys[15], part), 71), part)
    forget_gate_preact = draw_forget_gate_preact(jax.random.fold_in(jax.random.fold_in(keys[15], part), 71), part)
    forget_log_offset = draw_forget_log_offset(jax.random.fold_in(jax.random.fold_in(keys[15], part), 71), part)
    per_head_norm_gain = jnp.clip(1.0 + 0.18 * jax.random.normal(keys[6], (HEADS * DV,), jnp.float32), 0.099609375, 1.8984375).astype(jnp.bfloat16)
    cell_output_matrix = gaussian(keys[7], (HEADS * DV, D), (HEADS * DV) ** -0.5, 0.125, ((0, 4), (1, 32)))
    layer_input_rows = gaussian(own_keys[8], (TOKENS, D), 1.0, 6.0, ((0, 128),))
    expert_norm_gain = jnp.clip(1.0 + 0.18 * jax.random.normal(keys[9], (D,), jnp.float32), 0.099609375, 1.8984375).astype(jnp.bfloat16)
    chosen_expert_index_keys = jax.random.split(jax.random.fold_in(own_keys[10], 1), TOKENS // ROWS_DEV)
    chosen_expert_index_turns = jax.random.permutation(jax.random.fold_in(own_keys[10], 3), TOKENS // ROWS_DEV)
    chosen_expert_index = jax.vmap(lambda own, number: deal_out(jax.random.fold_in(own_keys[10], 2), own, number, ROWS_DEV, EXPERTS, 2, SLOTS, 2))(chosen_expert_index_keys, chosen_expert_index_turns).reshape((TOKENS, 2))
    chosen_expert_weight = jnp.clip(0.2 + 0.8 * jax.random.uniform(own_keys[11], (TOKENS, 2), jnp.float32) ** steps_of(own_keys[11], (TOKENS, 2), ((0, 128),), -0.2, 0.2), 0.2, 1.0)
    expert_gate_matrix = gaussian(keys[12], (EXPERTS, D, FF), D ** -0.5, 0.125, ((0, 32), (2, 4)))
    expert_up_matrix = gaussian(keys[13], (EXPERTS, D, FF), D ** -0.5, 0.125, ((0, 32), (2, 4)))
    expert_down_matrix = gaussian(keys[14], (EXPERTS, FF, D), FF ** -0.5, 0.09375, ((0, 32), (1, 4)))
    return dict(queries=queries, head_key_rows=head_key_rows, head_value_rows=head_value_rows, input_gate_logit=input_gate_logit, forget_gate_preact=forget_gate_preact, forget_log_offset=forget_log_offset, per_head_norm_gain=per_head_norm_gain, cell_output_matrix=cell_output_matrix, layer_input_rows=layer_input_rows, expert_norm_gain=expert_norm_gain, chosen_expert_index=chosen_expert_index, chosen_expert_weight=chosen_expert_weight, expert_gate_matrix=expert_gate_matrix, expert_up_matrix=expert_up_matrix, expert_down_matrix=expert_down_matrix)


far_below = -1e+30
norm_eps = 1e-06

def combine_states(earlier, later):
    total_a, memory_a, peak_a = earlier
    total_b, memory_b, peak_b = later
    peak = jnp.maximum(total_b + peak_a, peak_b)
    weight_a = jnp.exp(total_b + peak_a - peak)
    weight_b = jnp.exp(peak_b - peak)
    memory = weight_a[:, None, None] * memory_a + weight_b[:, None, None] * memory_b
    return (total_a + total_b, memory, peak)

def block_summary(keys3, values3, log_in, log_retention):
    running = jnp.cumsum(log_retention, axis=1)
    totals = running[:, -1]
    term_log = totals[:, None] - running + log_in
    peak = lax.optimization_barrier(jnp.max(term_log, axis=1))
    factors = jnp.transpose(jnp.exp(term_log - peak[:, None]))
    keys32 = keys3.astype(jnp.float32)
    weighted = values3.astype(jnp.float32) * factors[:, :, None]
    memory = jnp.einsum('shd,she->hde', keys32, weighted, precision=lax.Precision.HIGHEST)
    return (totals, memory, peak)

def block_output(queries3, keys3, values3, log_in, log_retention, state, gains):
    count = queries3.shape[0]
    heads = queries3.shape[1]
    memory_in, peak_in = (state[1], state[2])
    running = jnp.cumsum(log_retention, axis=1)
    rows_at = lax.broadcasted_iota(jnp.int32, (count, count), 0)
    cols_at = lax.broadcasted_iota(jnp.int32, (count, count), 1)
    causal = (cols_at <= rows_at)[None]
    decay_log = jnp.where(causal, running[:, :, None] - running[:, None, :] + log_in[:, None, :], far_below)
    carried_log = running + peak_in[:, None]
    peak = jnp.maximum(carried_log, lax.optimization_barrier(jnp.max(decay_log, axis=2)))
    qk_scale = queries3.shape[2] ** (-0.5)
    queries32 = queries3.astype(jnp.float32)
    scores = jnp.einsum('thd,shd->hts', queries32, keys3.astype(jnp.float32)) * qk_scale
    strength = scores * jnp.exp(decay_log - peak[:, :, None])
    carried = jnp.exp(carried_log - peak)
    from_memory = jnp.einsum('thd,hde->the', queries32, memory_in, precision=lax.Precision.HIGHEST) * qk_scale
    rounded = strength.astype(jnp.bfloat16).astype(jnp.float32)
    within = jnp.einsum('hts,she->the', rounded, values3.astype(jnp.float32))
    result = within + jnp.transpose(carried)[:, :, None] * from_memory
    result = result * lax.rsqrt(lax.optimization_barrier(jnp.mean(result * result, axis=2, keepdims=True)) + norm_eps)
    result = result * gains.astype(jnp.float32).reshape(heads, -1)
    return result.reshape(count, -1).astype(jnp.bfloat16)

def rounded_sum(left, right, groups):
    width = left.shape[1] // groups
    total = jnp.zeros((left.shape[0], right.shape[1]), jnp.float32)
    for group in range(groups):
        piece = jnp.dot(left[:, group * width:(group + 1) * width], right[group * width:(group + 1) * width], preferred_element_type=jnp.float32).astype(jnp.bfloat16)
        total = total + lax.optimization_barrier(piece).astype(jnp.float32)
    return total

def reference(queries, head_key_rows, head_value_rows, input_gate_logit, forget_gate_preact, forget_log_offset, per_head_norm_gain, cell_output_matrix, layer_input_rows, expert_norm_gain, chosen_expert_index, chosen_expert_weight, expert_gate_matrix, expert_up_matrix, expert_down_matrix):
    blocks = TOKENS // TOK_DEV
    log_retention = jax.nn.log_sigmoid(forget_gate_preact) + forget_log_offset
    queries_b = queries.reshape(blocks, TOK_DEV, HEADS, DK)
    keys_b = head_key_rows.reshape(blocks, TOK_DEV, HEADS, DK)
    values_b = head_value_rows.reshape(blocks, TOK_DEV, HEADS, DV)
    inputs_b = jnp.transpose(input_gate_logit.reshape(HEADS, blocks, TOK_DEV), (1, 0, 2))
    keeps_b = jnp.transpose(log_retention.reshape(HEADS, blocks, TOK_DEV), (1, 0, 2))
    start = (jnp.zeros((HEADS,), jnp.float32), jnp.zeros((HEADS, DK, DV), jnp.float32), jnp.full((HEADS,), far_below, jnp.float32))

    def advance(state, block):
        queries3, keys3, values3, log_in, keeps = block
        produced = block_output(queries3, keys3, values3, log_in, keeps, state, per_head_norm_gain)
        state = combine_states(state, block_summary(keys3, values3, log_in, keeps))
        return (state, produced)
    _, mixed = lax.scan(advance, start, (queries_b, keys_b, values_b, inputs_b, keeps_b))
    mixed = mixed.reshape(TOKENS, HEADS * DV)
    residual = layer_input_rows.astype(jnp.float32) + rounded_sum(mixed, cell_output_matrix, N_TP)
    normed = residual * lax.rsqrt(lax.optimization_barrier(jnp.mean(residual * residual, axis=1, keepdims=True)) + norm_eps)
    normed = (normed * expert_norm_gain.astype(jnp.float32)).astype(jnp.bfloat16)
    nblocks = TOKENS // ROWS_DEV
    pairs = chosen_expert_index.reshape(nblocks, ROWS_DEV * 2)
    onehot = (pairs[:, :, None] == jnp.arange(EXPERTS, dtype=jnp.int32)[None, None, :]).astype(jnp.int32)
    position = lax.optimization_barrier(jnp.sum(jnp.cumsum(onehot, axis=1) * onehot, axis=2)) - 1
    slot_index = (jnp.arange(nblocks, dtype=jnp.int32)[:, None] * SLOTS + position).reshape(TOKENS, 2)
    copies = jnp.broadcast_to(normed[:, None, :], (TOKENS, 2, D))
    buffer = jnp.zeros((EXPERTS, nblocks * SLOTS, D), jnp.bfloat16).at[chosen_expert_index, slot_index].set(copies)

    def run_expert(inputs):
        rows_in, gate_w, up_w, down_w = inputs
        gate = jnp.dot(rows_in, gate_w, preferred_element_type=jnp.float32)
        upward = jnp.dot(rows_in, up_w, preferred_element_type=jnp.float32)
        hidden = (jax.nn.silu(gate) * upward).astype(jnp.bfloat16)
        return rounded_sum(hidden, down_w, N_TP).astype(jnp.bfloat16)
    outputs = lax.map(run_expert, (buffer, expert_gate_matrix, expert_up_matrix, expert_down_matrix))
    picked = outputs[chosen_expert_index, slot_index].astype(jnp.float32)
    routed = lax.optimization_barrier(jnp.sum(chosen_expert_weight[:, :, None] * picked, axis=1))
    return (residual + routed).astype(jnp.bfloat16)
```

```python
import jax
import jax.numpy as jnp
from jax import lax
from jax.sharding import Mesh
from jax.sharding import PartitionSpec as P

DK = 64
DV = 128
SP = ("sp_0", "sp_1")
GRP_SP = ("grp", "sp_0", "sp_1")
GRP_SP_TP = ("grp", "sp_0", "sp_1", "tp")

far_below = -1e30
norm_eps = 1e-06
HIGHEST = lax.Precision.HIGHEST


def shifted(x, axis, by):
    size = lax.axis_size(axis)
    return lax.ppermute(x, axis, [(i, (i + by) % size) for i in range(size)])


def traded(x, axis):
    return lax.all_to_all(x, axis, split_axis=0, concat_axis=0, tiled=True)


def to_owners(memory, totals, peaks):
    heads, dk, dv = memory.shape
    chips = lax.axis_size("sp_0")
    half = heads // 2
    body = memory.reshape(2, half * dk, dv)
    head = jnp.concatenate([totals.reshape(2, half), peaks.reshape(2, half)], axis=1)
    head = jnp.pad(head, ((0, 0), (0, dv - 2 * half)))
    head = jnp.pad(head[:, None, :], ((0, 0), (0, 7), (0, 0)))
    mine = traded(jnp.concatenate([body, head], axis=1), "sp_1")
    rows = half * dk // chips
    body = mine[:, : half * dk].reshape(2, chips, rows, dv)
    body = jnp.transpose(body, (1, 0, 2, 3)).reshape(chips, 2 * rows, dv)
    head = jnp.broadcast_to(
        jnp.pad(mine[:, half * dk], ((0, 6), (0, 0)))[None], (chips, 8, dv)
    )
    got = traded(jnp.concatenate([body, head], axis=1), "sp_0")
    states = got[:, : 2 * rows].reshape(2 * chips, rows, dv)
    log_parts = got[:, 2 * rows : 2 * rows + 2, : 2 * half].reshape(2 * chips, 2 * half)
    which = lax.axis_index("sp_0") * rows // dk
    total = jnp.where(which == 0, log_parts[:, 0], log_parts[:, 1])
    peak = jnp.where(which == 0, log_parts[:, 2], log_parts[:, 3])
    return states, total, peak


def scan_slices(states, total, peak):
    size = total.shape[0]
    t = lax.broadcasted_iota(jnp.int32, (size, size), 0)
    s = lax.broadcasted_iota(jnp.int32, (size, size), 1)
    u = jnp.arange(size, dtype=jnp.int32)
    between = (u[None, None, :] > s[:, :, None]) & (u[None, None, :] < t[:, :, None])
    decay = jnp.sum(jnp.where(between, total[None, None, :], 0.0), axis=2)
    log_weight = jnp.where(s < t, decay + peak[None, :], far_below)
    top = jnp.max(log_weight, axis=1)
    weight = jnp.where(s < t, jnp.exp(log_weight - top[:, None]), 0.0)
    flat = states.reshape(size, -1)
    before = jnp.dot(weight, flat, precision=HIGHEST)
    return before.reshape(states.shape), top


def from_owners(before, top, heads, dk):
    size, rows, dv = before.shape
    chips = size // 2
    half = heads // 2
    body = before.reshape(chips, 2 * rows, dv)
    head = jnp.broadcast_to(top.reshape(chips, 2, 1), (chips, 2, dv))
    head = jnp.pad(head, ((0, 0), (0, 6), (0, 0)))
    got = traded(jnp.concatenate([body, head], axis=1), "sp_0")
    body = jnp.transpose(got[:, : 2 * rows].reshape(chips, 2, rows, dv), (1, 0, 2, 3))
    body = body.reshape(2, half * dk, dv)
    tops = got[:: chips // half, 2 * rows : 2 * rows + 2, :]
    tops = jnp.transpose(tops, (1, 0, 2))
    tops = jnp.pad(tops, ((0, 0), (0, 8 - half), (0, 0)))
    mine = traded(jnp.concatenate([body, tops], axis=1), "sp_1")
    memory = mine[:, : half * dk].reshape(heads, dk, dv)
    return memory, mine[:, half * dk : half * dk + half, 0].reshape(heads)


def expert_part(rows_in, gate_w, up_w, down_w):
    gate = jnp.dot(rows_in, gate_w, preferred_element_type=jnp.float32)
    upward = jnp.dot(rows_in, up_w, preferred_element_type=jnp.float32)
    hidden = (jax.nn.silu(gate) * upward).astype(jnp.bfloat16)
    return jnp.dot(hidden, down_w, preferred_element_type=jnp.float32).astype(jnp.bfloat16)


def shards(
    queries,
    head_key_rows,
    head_value_rows,
    input_gate_logit,
    forget_gate_preact,
    forget_log_offset,
    per_head_norm_gain,
    cell_output_matrix,
    layer_input_rows,
    expert_norm_gain,
    chosen_expert_index,
    chosen_expert_weight,
    expert_gate_matrix,
    expert_up_matrix,
    expert_down_matrix,
):
    count = queries.shape[0]
    heads = input_gate_logit.shape[0]
    queries3 = queries.reshape(count, heads, DK)
    keys3 = head_key_rows.reshape(count, heads, DK)
    values3 = head_value_rows.reshape(count, heads, DV)
    rows_at = lax.broadcasted_iota(jnp.int32, (count, count), 0)
    cols_at = lax.broadcasted_iota(jnp.int32, (count, count), 1)
    causal = cols_at <= rows_at

    log_retention = jax.nn.log_sigmoid(forget_gate_preact) + forget_log_offset
    running = jnp.dot(log_retention, (rows_at <= cols_at).astype(jnp.float32), precision=HIGHEST)
    totals = running[:, -1]
    term_log = totals[:, None] - running + input_gate_logit
    own_peak = jnp.max(term_log, axis=1)
    factors = jnp.transpose(jnp.exp(term_log - own_peak[:, None]))
    weighted = values3.astype(jnp.float32) * factors[:, :, None]
    own_memory = jnp.einsum(
        "shd,she->hde", keys3.astype(jnp.float32), weighted, precision=HIGHEST
    )

    states, total, peak = to_owners(own_memory, totals, own_peak)
    before, top = scan_slices(states, total, peak)
    memory_in, peak_in = from_owners(before, top, heads, DK)

    decay_log = jnp.where(
        causal[None],
        running[:, :, None] - running[:, None, :] + input_gate_logit[:, None, :],
        far_below,
    )
    carried_log = running + peak_in[:, None]
    peak = jnp.maximum(carried_log, jnp.max(decay_log, axis=2))
    qk_scale = DK ** (-0.5)
    scores = (
        jnp.einsum("thd,shd->hts", queries3, keys3, preferred_element_type=jnp.float32) * qk_scale
    )
    strength = scores * jnp.exp(decay_log - peak[:, :, None])
    carried = jnp.exp(carried_log - peak)
    from_memory = (
        jnp.einsum("thd,hde->the", queries3.astype(jnp.float32), memory_in, precision=HIGHEST)
        * qk_scale
    )
    within = jnp.einsum(
        "hts,she->the", strength.astype(jnp.bfloat16), values3, preferred_element_type=jnp.float32
    )
    result = within + jnp.transpose(carried)[:, :, None] * from_memory
    result = result * lax.rsqrt(jnp.mean(result * result, axis=2, keepdims=True) + norm_eps)
    result = result * per_head_norm_gain.astype(jnp.float32).reshape(heads, -1)
    mixed = result.reshape(count, -1).astype(jnp.bfloat16)

    partial_value = jnp.dot(
        mixed,
        lax.all_gather(cell_output_matrix, SP, axis=1, tiled=True),
        preferred_element_type=jnp.float32,
    ).astype(jnp.bfloat16)
    rows, width = layer_input_rows.shape
    tiles = traded(partial_value.reshape(lax.axis_size("tp"), rows, width), "tp")
    residual = layer_input_rows.astype(jnp.float32) + jnp.sum(tiles.astype(jnp.float32), axis=0)
    normed = residual * lax.rsqrt(jnp.mean(residual * residual, axis=1, keepdims=True) + norm_eps)
    normed = (normed * expert_norm_gain.astype(jnp.float32)).astype(jnp.bfloat16)

    experts = lax.axis_size(SP)
    slots = (4 * rows + experts - 1) // experts
    expert_at = jnp.arange(experts, dtype=jnp.int32)[None, :]
    named = [
        (chosen_expert_index[:, k : k + 1] == expert_at).astype(jnp.bfloat16) for k in range(2)
    ]
    below = (
        lax.broadcasted_iota(jnp.int32, (rows, rows), 1)
        < lax.broadcasted_iota(jnp.int32, (rows, rows), 0)
    ).astype(jnp.bfloat16)
    ahead = [jnp.dot(below, n, preferred_element_type=jnp.float32) for n in named]
    first = jnp.sum(named[0].astype(jnp.float32), axis=0, keepdims=True)
    ahead[1] = ahead[1] + first
    picks = []
    for k in range(2):
        place = jnp.sum(named[k].astype(jnp.float32) * ahead[k], axis=1, keepdims=True)
        slot = chosen_expert_index[:, k : k + 1] * slots + place.astype(jnp.int32)
        target = lax.broadcasted_iota(jnp.int32, (rows, experts * slots), 1)
        picks.append((slot == target).astype(jnp.bfloat16))
    outgoing = lax.dot_general(
        picks[0] + picks[1],
        normed,
        (((0,), (0,)), ((), ())),
        preferred_element_type=jnp.float32,
    ).astype(jnp.bfloat16)

    arrived = traded(outgoing.reshape(experts, slots, width), SP)
    arrived = jnp.transpose(arrived, (1, 0, 2)).reshape(slots * experts, width)
    weights = (expert_gate_matrix[0], expert_up_matrix[0], expert_down_matrix[0])
    size = lax.axis_size("tp")
    spread = {by: shifted(arrived, "tp", by) for by in (1, size - 1, 2)}
    total_out = expert_part(arrived, *weights).astype(jnp.float32)
    for by in (1, size - 1, 2):
        total_out = total_out + shifted(
            expert_part(spread[by], *weights), "tp", size - by
        ).astype(jnp.float32)
    expert_out = total_out.astype(jnp.bfloat16).reshape(slots, experts, width)
    back = traded(jnp.transpose(expert_out, (1, 0, 2)), SP)
    flat_out = back.reshape(experts * slots, width)

    out = residual
    for k in range(2):
        picked = jnp.dot(picks[k], flat_out, preferred_element_type=jnp.float32)
        out = out + chosen_expert_weight[:, k : k + 1] * picked
    return out.astype(jnp.bfloat16)


def solution(mesh):
    torus = Mesh(
        mesh.devices.reshape(mesh.shape["grp"], mesh.shape["sp"] // 2, 2, mesh.shape["tp"]),
        ("grp", "sp_0", "sp_1", "tp"),
    )
    return jax.shard_map(
        shards,
        mesh=torus,
        in_specs=(
            P(GRP_SP, "tp"),
            P(GRP_SP, "tp"),
            P(GRP_SP, "tp"),
            P("tp", GRP_SP),
            P("tp", GRP_SP),
            P("tp", GRP_SP),
            P("tp"),
            P("tp", SP),
            P(GRP_SP_TP, None),
            P(),
            P(GRP_SP_TP, None),
            P(GRP_SP_TP, None),
            P(SP, None, "tp"),
            P(SP, None, "tp"),
            P(SP, "tp", None),
        ),
        out_specs=P(GRP_SP_TP, None),
        check_vma=False,
    )
```

```python
import jax
import jax.numpy as jnp
from jax import lax
from jax.sharding import Mesh
from jax.sharding import PartitionSpec as P


DK = 64
DV = 128
NEAR = ("near", "core")
SP = ("far", *NEAR)
GRP_SP = ("grp", *SP)
GRP_SP_TP = (*GRP_SP, "tp")

far_below = -1e30
norm_eps = 1e-06
HIGHEST = lax.Precision.HIGHEST


def shifted(x, axis, by):
    size = lax.axis_size(axis)
    return lax.ppermute(x, axis, [(i, (i + by) % size) for i in range(size)])


def traded(x, axis):
    return lax.all_to_all(x, axis, split_axis=0, concat_axis=0, tiled=True)


def strength_of(totals, peaks):
    size = totals.shape[0]
    shape = (size + 1, size, size)
    t, s, u = (lax.broadcasted_iota(jnp.int32, shape, d) for d in range(3))
    decay = jnp.sum(jnp.where((s < u) & (u < t), totals[None, None, :], 0.0), axis=2)
    earlier = s[:, :, 0] < t[:, :, 0]
    logs = jnp.where(earlier, decay + peaks[None, :], far_below)
    tops = jnp.max(logs, axis=1)
    return jnp.where(earlier, jnp.exp(logs - tops[:, None]), 0.0), tops


def with_header(body, *scalars):
    count, _, lanes = body.shape
    lines = [jnp.broadcast_to(x.reshape(count, 1, 1), (count, 1, lanes)) for x in scalars]
    lines.append(jnp.zeros((count, 8 - len(scalars), lanes), jnp.float32))
    return jnp.concatenate([body, *lines], axis=1)


def states_before(memory, totals, peaks):
    heads, dk, dv = memory.shape
    near = lax.axis_size(NEAR)
    far = lax.axis_size("far")
    rows = heads * dk // near
    per_head = near // heads
    sent = with_header(
        memory.reshape(near, rows, dv), jnp.repeat(totals, per_head), jnp.repeat(peaks, per_head)
    )
    got = traded(sent, NEAR)
    parts, total, peak = got[:, :rows], got[:, rows, 0], got[:, rows + 1, 0]
    size = total.shape[0]
    weight, tops = strength_of(total, peak)
    whole = jnp.sum(weight[size][:, None, None] * parts, axis=0)
    whole = with_header(whole[None], jnp.sum(total).reshape(1), tops[size].reshape(1))[0]
    group = lax.axis_index("far")
    before = []
    for back in range(far - 1, 0, -1):
        other = lax.ppermute(whole, "far", [(i, i + back) for i in range(far - back)])
        before.append(jnp.where(group >= back, other, jnp.zeros_like(other)))
    stack = jnp.stack(before)
    known = group >= jnp.arange(far - 1, 0, -1)
    all_total = jnp.concatenate([stack[:, rows, 0], total])
    all_peak = jnp.concatenate([jnp.where(known, stack[:, rows + 1, 0], far_below), peak])
    weight, tops = strength_of(all_total, all_peak)
    weight, tops = weight[far - 1 : -1], tops[far - 1 : -1]
    states = jnp.concatenate([stack[:, :rows], parts], axis=0)
    states = jnp.sum(weight[:, :, None, None] * states[None], axis=1)
    mine = traded(with_header(states, tops), NEAR)
    return mine[:, :rows].reshape(heads, dk, dv), mine[::per_head, rows, 0]


def gathered_columns(matrix):
    own = jnp.transpose(matrix)
    far, near = lax.axis_size("far"), lax.axis_size("near")
    level = jnp.stack([own] + [shifted(own, "far", far - i) for i in range(1, far)])
    chips = far * near
    wide = []
    for k in (-1, 0, 1, 2):
        if k:
            wide.append(shifted(level, ("far", "near"), chips - k))
        else:
            wide.append(level)
    mine = jnp.stack(wide, axis=1).reshape(chips, *own.shape)
    other = shifted(mine, "core", 1)
    core = lax.axis_index("core")
    both = jnp.stack([jnp.where(core == 0, mine, other), jnp.where(core == 0, other, mine)], axis=1)
    both = both.reshape(chips, -1, own.shape[1])
    both = jnp.concatenate([both, both], axis=0)
    at = lax.axis_index(("far", "near"))
    start = jnp.where(at == 0, 1, chips + 1 - at)
    whole = lax.dynamic_slice_in_dim(both, start, chips, axis=0)
    return whole.reshape(-1, own.shape[1])


def expert_part(rows_in, gate_w, up_w, down_w):
    gate = jnp.dot(rows_in, gate_w, preferred_element_type=jnp.float32)
    upward = jnp.dot(rows_in, up_w, preferred_element_type=jnp.float32)
    hidden = (jax.nn.silu(gate) * upward).astype(jnp.bfloat16)
    return jnp.dot(hidden, down_w, preferred_element_type=jnp.float32).astype(jnp.bfloat16)


def shards(
    queries,
    head_key_rows,
    head_value_rows,
    input_gate_logit,
    forget_gate_preact,
    forget_log_offset,
    per_head_norm_gain,
    cell_output_matrix,
    layer_input_rows,
    expert_norm_gain,
    chosen_expert_index,
    chosen_expert_weight,
    expert_gate_matrix,
    expert_up_matrix,
    expert_down_matrix,
):
    count = queries.shape[0]
    heads = input_gate_logit.shape[0]
    queries3 = queries.reshape(count, heads, DK)
    keys3 = head_key_rows.reshape(count, heads, DK)
    values3 = head_value_rows.reshape(count, heads, DV)
    rows_at = lax.broadcasted_iota(jnp.int32, (count, count), 0)
    cols_at = lax.broadcasted_iota(jnp.int32, (count, count), 1)
    causal = cols_at <= rows_at

    log_retention = jax.nn.log_sigmoid(forget_gate_preact) + forget_log_offset
    running = jnp.dot(log_retention, (rows_at <= cols_at).astype(jnp.float32), precision=HIGHEST)
    totals = running[:, -1]
    term_log = totals[:, None] - running + input_gate_logit
    own_peak = jnp.max(term_log, axis=1)
    factors = jnp.transpose(jnp.exp(term_log - own_peak[:, None]))
    weighted = values3.astype(jnp.float32) * factors[:, :, None]
    own_memory = jnp.einsum(
        "shd,she->hde", keys3.astype(jnp.float32), weighted, precision=HIGHEST
    )

    memory_in, peak_in = states_before(own_memory, totals, own_peak)

    decay_log = jnp.where(
        causal[None],
        running[:, :, None] - running[:, None, :] + input_gate_logit[:, None, :],
        far_below,
    )
    carried_log = running + peak_in[:, None]
    peak = jnp.maximum(carried_log, jnp.max(decay_log, axis=2))
    qk_scale = DK ** (-0.5)
    scores = (
        jnp.einsum("thd,shd->hts", queries3, keys3, preferred_element_type=jnp.float32) * qk_scale
    )
    strength = scores * jnp.exp(decay_log - peak[:, :, None])
    carried = jnp.exp(carried_log - peak)
    from_memory = (
        jnp.einsum("thd,hde->the", queries3.astype(jnp.float32), memory_in, precision=HIGHEST)
        * qk_scale
    )
    within = jnp.einsum(
        "hts,she->the", strength.astype(jnp.bfloat16), values3, preferred_element_type=jnp.float32
    )
    result = within + jnp.transpose(carried)[:, :, None] * from_memory
    result = result * lax.rsqrt(jnp.mean(result * result, axis=2, keepdims=True) + norm_eps)
    result = result * per_head_norm_gain.astype(jnp.float32).reshape(heads, -1)
    mixed = result.reshape(count, -1).astype(jnp.bfloat16)

    partial_value = lax.dot_general(
        mixed,
        gathered_columns(cell_output_matrix),
        (((1,), (1,)), ((), ())),
        preferred_element_type=jnp.float32,
    ).astype(jnp.bfloat16)
    rows, width = layer_input_rows.shape
    tiles = traded(partial_value.reshape(lax.axis_size("tp"), rows, width), "tp")
    residual = layer_input_rows.astype(jnp.float32) + jnp.sum(tiles.astype(jnp.float32), axis=0)
    normed = residual * lax.rsqrt(jnp.mean(residual * residual, axis=1, keepdims=True) + norm_eps)
    normed = (normed * expert_norm_gain.astype(jnp.float32)).astype(jnp.bfloat16)

    experts = lax.axis_size(SP)
    slots = (4 * rows + experts - 1) // experts
    expert_at = jnp.arange(experts, dtype=jnp.int32)[None, :]
    named = [
        (chosen_expert_index[:, k : k + 1] == expert_at).astype(jnp.bfloat16) for k in range(2)
    ]
    below = (
        lax.broadcasted_iota(jnp.int32, (rows, rows), 1)
        < lax.broadcasted_iota(jnp.int32, (rows, rows), 0)
    ).astype(jnp.bfloat16)
    ahead = [jnp.dot(below, n, preferred_element_type=jnp.float32) for n in named]
    first = jnp.sum(named[0].astype(jnp.float32), axis=0, keepdims=True)
    ahead[1] = ahead[1] + first
    picks = []
    for k in range(2):
        place = jnp.sum(named[k].astype(jnp.float32) * ahead[k], axis=1, keepdims=True)
        slot = chosen_expert_index[:, k : k + 1] * slots + place.astype(jnp.int32)
        target = lax.broadcasted_iota(jnp.int32, (rows, experts * slots), 1)
        picks.append((slot == target).astype(jnp.bfloat16))
    outgoing = lax.dot_general(
        picks[0] + picks[1],
        normed,
        (((0,), (0,)), ((), ())),
        preferred_element_type=jnp.float32,
    ).astype(jnp.bfloat16)

    arrived = traded(outgoing.reshape(experts, slots, width), SP)
    arrived = jnp.transpose(arrived, (1, 0, 2)).reshape(slots * experts, width)
    weights = (expert_gate_matrix[0], expert_up_matrix[0], expert_down_matrix[0])
    size = lax.axis_size("tp")
    half = arrived.shape[0] // 2
    left = shifted(arrived, "tp", 1)
    right = shifted(arrived, "tp", size - 1)
    own = expert_part(arrived, *weights)
    across = [shifted(left[:half], "tp", 1), shifted(right[half:], "tp", size - 1)]
    left, right, _ = lax.optimization_barrier((left, right, own))
    from_left = expert_part(left, *weights)
    parts = [own, shifted(from_left, "tp", size - 1)]
    right, _ = lax.optimization_barrier((right, from_left))
    from_right = expert_part(right, *weights)
    parts.append(shifted(from_right, "tp", 1))
    across, _ = lax.optimization_barrier((jnp.concatenate(across, axis=0), from_right))
    from_across = expert_part(across, *weights)
    parts.append(shifted(from_across, "tp", 2))
    total_out = sum(part.astype(jnp.float32) for part in parts)
    expert_out = total_out.astype(jnp.bfloat16).reshape(slots, experts, width)
    back = traded(jnp.transpose(expert_out, (1, 0, 2)), SP)
    flat_out = back.reshape(experts * slots, width)

    out = residual
    for k in range(2):
        picked = jnp.dot(picks[k], flat_out, preferred_element_type=jnp.float32)
        out = out + chosen_expert_weight[:, k : k + 1] * picked
    return out.astype(jnp.bfloat16)


def solution(mesh):
    sp = mesh.shape["sp"]
    torus = Mesh(
        mesh.devices.reshape(mesh.shape["grp"], sp // 8, 4, 2, mesh.shape["tp"]), GRP_SP_TP
    )
    return jax.shard_map(
        shards,
        mesh=torus,
        in_specs=(
            P(GRP_SP, "tp"),
            P(GRP_SP, "tp"),
            P(GRP_SP, "tp"),
            P("tp", GRP_SP),
            P("tp", GRP_SP),
            P("tp", GRP_SP),
            P("tp"),
            P("tp", SP),
            P(GRP_SP_TP, None),
            P(),
            P(GRP_SP_TP, None),
            P(GRP_SP_TP, None),
            P(SP, None, "tp"),
            P(SP, None, "tp"),
            P(SP, "tp", None),
        ),
        out_specs=P(GRP_SP_TP, None),
        check_vma=False,
    )
```

```python
import jax
import jax.numpy as jnp
from jax import lax
from jax.experimental import pallas as pl
from jax.experimental.pallas import tpu as pltpu
from jax.sharding import Mesh
from jax.sharding import PartitionSpec as P


DK = 64
DV = 128
NEAR = ("near", "core")
SP = ("far", *NEAR)
GRP_SP = ("grp", *SP)
GRP_SP_TP = (*GRP_SP, "tp")

far_below = -1e30
norm_eps = 1e-06
HIGHEST = lax.Precision.HIGHEST


def shifted(x, axis, by):
    size = lax.axis_size(axis)
    return lax.ppermute(x, axis, [(i, (i + by) % size) for i in range(size)])


def traded(x, axis):
    return lax.all_to_all(x, axis, split_axis=0, concat_axis=0, tiled=True)


def strength_of(totals, peaks):
    size = totals.shape[0]
    shape = (size + 1, size, size)
    t, s, u = (lax.broadcasted_iota(jnp.int32, shape, d) for d in range(3))
    decay = jnp.sum(jnp.where((s < u) & (u < t), totals[None, None, :], 0.0), axis=2)
    earlier = s[:, :, 0] < t[:, :, 0]
    logs = jnp.where(earlier, decay + peaks[None, :], far_below)
    tops = jnp.max(logs, axis=1)
    return jnp.where(earlier, jnp.exp(logs - tops[:, None]), 0.0), tops


def with_header(body, *scalars):
    count, _, lanes = body.shape
    lines = [jnp.broadcast_to(x.reshape(count, 1, 1), (count, 1, lanes)) for x in scalars]
    lines.append(jnp.zeros((count, 8 - len(scalars), lanes), jnp.float32))
    return jnp.concatenate([body, *lines], axis=1)


def states_before(memory, totals, peaks):
    heads, dk, dv = memory.shape
    near = lax.axis_size(NEAR)
    far = lax.axis_size("far")
    rows = heads * dk // near
    per_head = near // heads
    sent = with_header(
        memory.reshape(near, rows, dv), jnp.repeat(totals, per_head), jnp.repeat(peaks, per_head)
    )
    got = traded(sent, NEAR)
    parts, total, peak = got[:, :rows], got[:, rows, 0], got[:, rows + 1, 0]
    size = total.shape[0]
    weight, tops = strength_of(total, peak)
    whole = jnp.sum(weight[size][:, None, None] * parts, axis=0)
    whole = with_header(whole[None], jnp.sum(total).reshape(1), tops[size].reshape(1))[0]
    group = lax.axis_index("far")
    before = []
    for back in range(far - 1, 0, -1):
        other = lax.ppermute(whole, "far", [(i, i + back) for i in range(far - back)])
        before.append(jnp.where(group >= back, other, jnp.zeros_like(other)))
    stack = jnp.stack(before)
    known = group >= jnp.arange(far - 1, 0, -1)
    all_total = jnp.concatenate([stack[:, rows, 0], total])
    all_peak = jnp.concatenate([jnp.where(known, stack[:, rows + 1, 0], far_below), peak])
    weight, tops = strength_of(all_total, all_peak)
    weight, tops = weight[far - 1 : -1], tops[far - 1 : -1]
    states = jnp.concatenate([stack[:, :rows], parts], axis=0)
    states = jnp.sum(weight[:, :, None, None] * states[None], axis=1)
    mine = traded(with_header(states, tops), NEAR)
    return mine[:, :rows].reshape(heads, dk, dv), mine[::per_head, rows, 0]


def gathered_columns(matrix):
    own = jnp.transpose(matrix)
    far, near = lax.axis_size("far"), lax.axis_size("near")
    level = jnp.stack([own] + [shifted(own, "far", far - i) for i in range(1, far)])
    chips = far * near
    wide = []
    for k in (-1, 0, 1, 2):
        if k:
            wide.append(shifted(level, ("far", "near"), chips - k))
        else:
            wide.append(level)
    mine = jnp.stack(wide, axis=1).reshape(chips, *own.shape)
    other = shifted(mine, "core", 1)
    core = lax.axis_index("core")
    both = jnp.stack([jnp.where(core == 0, mine, other), jnp.where(core == 0, other, mine)], axis=1)
    both = both.reshape(chips, -1, own.shape[1])
    both = jnp.concatenate([both, both], axis=0)
    at = lax.axis_index(("far", "near"))
    start = jnp.where(at == 0, 1, chips + 1 - at)
    whole = lax.dynamic_slice_in_dim(both, start, chips, axis=0)
    return whole.reshape(-1, own.shape[1])


def expert_body(units, rows_ref, gate_ref, up_ref, down_ref, out_ref, hidden_ref):
    step = pl.program_id(0)

    @pl.when(step < units)
    def _():
        both = jnp.concatenate([gate_ref[...], up_ref[...]], axis=1)
        made = jnp.dot(rows_ref[...], both, preferred_element_type=jnp.float32)
        gate, upward = made[:, : gate_ref.shape[1]], made[:, gate_ref.shape[1] :]
        hidden = gate / (1.0 + jnp.exp(-gate)) * upward
        at = pl.multiple_of(step * gate_ref.shape[1], gate_ref.shape[1])
        hidden_ref[:, pl.ds(at, gate_ref.shape[1])] = hidden.astype(jnp.bfloat16)

    @pl.when(step >= units)
    def _():
        out_ref[...] = jnp.dot(
            hidden_ref[...], down_ref[...], preferred_element_type=jnp.float32
        ).astype(jnp.bfloat16)


def expert_part(rows_in, gate_w, up_w, down_w):
    count, width = rows_in.shape
    inner = gate_w.shape[1]
    unit, wide = 128, 512
    units, columns = inner // unit, width // wide
    return pl.pallas_call(
        lambda *refs: expert_body(units, *refs),
        grid=(units + columns,),
        in_specs=[
            pl.BlockSpec((count, width), lambda i: (0, 0)),
            pl.BlockSpec((width, unit), lambda i: (0, jnp.minimum(i, units - 1))),
            pl.BlockSpec((width, unit), lambda i: (0, jnp.minimum(i, units - 1))),
            pl.BlockSpec((inner, wide), lambda i: (0, jnp.maximum(i - units, 0))),
        ],
        out_specs=pl.BlockSpec((count, wide), lambda i: (0, jnp.maximum(i - units, 0))),
        out_shape=jax.ShapeDtypeStruct((count, width), jnp.bfloat16),
        scratch_shapes=[pltpu.VMEM((count, inner), jnp.bfloat16)],
        compiler_params=pltpu.CompilerParams(dimension_semantics=("arbitrary",)),
        cost_estimate=pl.CostEstimate(
            flops=6 * count * width * inner,
            bytes_accessed=6 * width * inner + 4 * count * width,
            transcendentals=count * inner,
        ),
        name="expert_part",
    )(rows_in, gate_w, up_w, down_w)


def shards(
    queries,
    head_key_rows,
    head_value_rows,
    input_gate_logit,
    forget_gate_preact,
    forget_log_offset,
    per_head_norm_gain,
    cell_output_matrix,
    layer_input_rows,
    expert_norm_gain,
    chosen_expert_index,
    chosen_expert_weight,
    expert_gate_matrix,
    expert_up_matrix,
    expert_down_matrix,
):
    count = queries.shape[0]
    heads = input_gate_logit.shape[0]
    queries3 = queries.reshape(count, heads, DK)
    keys3 = head_key_rows.reshape(count, heads, DK)
    values3 = head_value_rows.reshape(count, heads, DV)
    rows_at = lax.broadcasted_iota(jnp.int32, (count, count), 0)
    cols_at = lax.broadcasted_iota(jnp.int32, (count, count), 1)
    causal = cols_at <= rows_at

    log_retention = jax.nn.log_sigmoid(forget_gate_preact) + forget_log_offset
    running = jnp.dot(log_retention, (rows_at <= cols_at).astype(jnp.float32), precision=HIGHEST)
    totals = running[:, -1]
    term_log = totals[:, None] - running + input_gate_logit
    own_peak = jnp.max(term_log, axis=1)
    factors = jnp.transpose(jnp.exp(term_log - own_peak[:, None]))
    weighted = values3.astype(jnp.float32) * factors[:, :, None]
    own_memory = jnp.einsum(
        "shd,she->hde", keys3.astype(jnp.float32), weighted, precision=HIGHEST
    )

    memory_in, peak_in = states_before(own_memory, totals, own_peak)

    decay_log = jnp.where(
        causal[None],
        running[:, :, None] - running[:, None, :] + input_gate_logit[:, None, :],
        far_below,
    )
    carried_log = running + peak_in[:, None]
    peak = jnp.maximum(carried_log, jnp.max(decay_log, axis=2))
    qk_scale = DK ** (-0.5)
    scores = (
        jnp.einsum("thd,shd->hts", queries3, keys3, preferred_element_type=jnp.float32) * qk_scale
    )
    strength = scores * jnp.exp(decay_log - peak[:, :, None])
    carried = jnp.exp(carried_log - peak)
    from_memory = (
        jnp.einsum("thd,hde->the", queries3.astype(jnp.float32), memory_in, precision=HIGHEST)
        * qk_scale
    )
    within = jnp.einsum(
        "hts,she->the", strength.astype(jnp.bfloat16), values3, preferred_element_type=jnp.float32
    )
    result = within + jnp.transpose(carried)[:, :, None] * from_memory
    result = result * lax.rsqrt(jnp.mean(result * result, axis=2, keepdims=True) + norm_eps)
    result = result * per_head_norm_gain.astype(jnp.float32).reshape(heads, -1)
    mixed = result.reshape(count, -1).astype(jnp.bfloat16)

    partial_value = lax.dot_general(
        mixed,
        gathered_columns(cell_output_matrix),
        (((1,), (1,)), ((), ())),
        preferred_element_type=jnp.float32,
    ).astype(jnp.bfloat16)
    rows, width = layer_input_rows.shape
    tiles = traded(partial_value.reshape(lax.axis_size("tp"), rows, width), "tp")
    residual = layer_input_rows.astype(jnp.float32) + jnp.sum(tiles.astype(jnp.float32), axis=0)
    normed = residual * lax.rsqrt(jnp.mean(residual * residual, axis=1, keepdims=True) + norm_eps)
    normed = (normed * expert_norm_gain.astype(jnp.float32)).astype(jnp.bfloat16)

    experts = lax.axis_size(SP)
    slots = (4 * rows + experts - 1) // experts
    expert_at = jnp.arange(experts, dtype=jnp.int32)[None, :]
    named = [
        (chosen_expert_index[:, k : k + 1] == expert_at).astype(jnp.bfloat16) for k in range(2)
    ]
    below = (
        lax.broadcasted_iota(jnp.int32, (rows, rows), 1)
        < lax.broadcasted_iota(jnp.int32, (rows, rows), 0)
    ).astype(jnp.bfloat16)
    ahead = [jnp.dot(below, n, preferred_element_type=jnp.float32) for n in named]
    first = jnp.sum(named[0].astype(jnp.float32), axis=0, keepdims=True)
    ahead[1] = ahead[1] + first
    picks = []
    for k in range(2):
        place = jnp.sum(named[k].astype(jnp.float32) * ahead[k], axis=1, keepdims=True)
        slot = chosen_expert_index[:, k : k + 1] * slots + place.astype(jnp.int32)
        target = lax.broadcasted_iota(jnp.int32, (rows, experts * slots), 1)
        picks.append((slot == target).astype(jnp.bfloat16))
    outgoing = lax.dot_general(
        picks[0] + picks[1],
        normed,
        (((0,), (0,)), ((), ())),
        preferred_element_type=jnp.float32,
    ).astype(jnp.bfloat16)

    arrived = traded(outgoing.reshape(experts, slots, width), SP)
    arrived = jnp.transpose(arrived, (1, 0, 2)).reshape(slots * experts, width)
    weights = (expert_gate_matrix[0], expert_up_matrix[0], expert_down_matrix[0])
    size = lax.axis_size("tp")
    half = arrived.shape[0] // 2
    left = shifted(arrived, "tp", 1)
    right = shifted(arrived, "tp", size - 1)
    own = expert_part(arrived, *weights)
    across = [shifted(left[:half], "tp", 1), shifted(right[half:], "tp", size - 1)]
    left, right, _ = lax.optimization_barrier((left, right, own))
    from_left = expert_part(left, *weights)
    right, _ = lax.optimization_barrier((right, from_left))
    from_right = expert_part(right, *weights)
    across, _ = lax.optimization_barrier((jnp.concatenate(across, axis=0), from_right))
    from_across = expert_part(across, *weights)
    parts = [
        own,
        shifted(from_left, "tp", size - 1),
        shifted(from_right, "tp", 1),
        shifted(from_across, "tp", 2),
    ]
    total_out = sum(part.astype(jnp.float32) for part in parts)
    expert_out = total_out.astype(jnp.bfloat16).reshape(slots, experts, width)
    back = traded(jnp.transpose(expert_out, (1, 0, 2)), SP)
    flat_out = back.reshape(experts * slots, width)

    out = residual
    for k in range(2):
        picked = jnp.dot(picks[k], flat_out, preferred_element_type=jnp.float32)
        out = out + chosen_expert_weight[:, k : k + 1] * picked
    return out.astype(jnp.bfloat16)


def solution(mesh):
    sp = mesh.shape["sp"]
    torus = Mesh(
        mesh.devices.reshape(mesh.shape["grp"], sp // 8, 4, 2, mesh.shape["tp"]), GRP_SP_TP
    )
    return jax.shard_map(
        shards,
        mesh=torus,
        in_specs=(
            P(GRP_SP, "tp"),
            P(GRP_SP, "tp"),
            P(GRP_SP, "tp"),
            P("tp", GRP_SP),
            P("tp", GRP_SP),
            P("tp", GRP_SP),
            P("tp"),
            P("tp", SP),
            P(GRP_SP_TP, None),
            P(),
            P(GRP_SP_TP, None),
            P(GRP_SP_TP, None),
            P(SP, None, "tp"),
            P(SP, None, "tp"),
            P(SP, "tp", None),
        ),
        out_specs=P(GRP_SP_TP, None),
        check_vma=False,
    )
```

```python
import jax
import jax.numpy as jnp
from jax import lax
from jax.experimental import pallas as pl
from jax.experimental.pallas import tpu as pltpu
from jax.sharding import Mesh
from jax.sharding import PartitionSpec as P


DK = 64
DV = 128
NEAR = ("near", "core")
SP = ("far", *NEAR)
GRP_SP = ("grp", *SP)
GRP_SP_TP = (*GRP_SP, "tp")

far_below = -1e30
norm_eps = 1e-06
HIGHEST = lax.Precision.HIGHEST


def shifted(x, axis, by):
    size = lax.axis_size(axis)
    return lax.ppermute(x, axis, [(i, (i + by) % size) for i in range(size)])


def traded(x, axis):
    return lax.all_to_all(x, axis, split_axis=0, concat_axis=0, tiled=True)


def strength_of(totals, peaks):
    size = totals.shape[0]
    shape = (size + 1, size, size)
    t, s, u = (lax.broadcasted_iota(jnp.int32, shape, d) for d in range(3))
    decay = jnp.sum(jnp.where((s < u) & (u < t), totals[None, None, :], 0.0), axis=2)
    earlier = s[:, :, 0] < t[:, :, 0]
    logs = jnp.where(earlier, decay + peaks[None, :], far_below)
    tops = jnp.max(logs, axis=1)
    return jnp.where(earlier, jnp.exp(logs - tops[:, None]), 0.0), tops


def with_header(body, *scalars):
    count, _, lanes = body.shape
    lines = [jnp.broadcast_to(x.reshape(count, 1, 1), (count, 1, lanes)) for x in scalars]
    lines.append(jnp.zeros((count, 8 - len(scalars), lanes), jnp.float32))
    return jnp.concatenate([body, *lines], axis=1)


def states_before(memory, totals, peaks):
    heads, dk, dv = memory.shape
    near = lax.axis_size(NEAR)
    far = lax.axis_size("far")
    rows = heads * dk // near
    per_head = near // heads
    sent = with_header(
        memory.reshape(near, rows, dv), jnp.repeat(totals, per_head), jnp.repeat(peaks, per_head)
    )
    got = traded(sent, NEAR)
    parts, total, peak = got[:, :rows], got[:, rows, 0], got[:, rows + 1, 0]
    size = total.shape[0]
    weight, tops = strength_of(total, peak)
    whole = jnp.sum(weight[size][:, None, None] * parts, axis=0)
    whole = with_header(whole[None], jnp.sum(total).reshape(1), tops[size].reshape(1))[0]
    group = lax.axis_index("far")
    before = []
    for back in range(far - 1, 0, -1):
        other = lax.ppermute(whole, "far", [(i, i + back) for i in range(far - back)])
        before.append(jnp.where(group >= back, other, jnp.zeros_like(other)))
    stack = jnp.stack(before)
    known = group >= jnp.arange(far - 1, 0, -1)
    all_total = jnp.concatenate([stack[:, rows, 0], total])
    all_peak = jnp.concatenate([jnp.where(known, stack[:, rows + 1, 0], far_below), peak])
    weight, tops = strength_of(all_total, all_peak)
    weight, tops = weight[far - 1 : -1], tops[far - 1 : -1]
    states = jnp.concatenate([stack[:, :rows], parts], axis=0)
    states = jnp.sum(weight[:, :, None, None] * states[None], axis=1)
    mine = traded(with_header(states, tops), NEAR)
    return mine[:, :rows].reshape(heads, dk, dv), mine[::per_head, rows, 0]


def gathered_columns(matrix):
    own = jnp.transpose(matrix)
    far, near = lax.axis_size("far"), lax.axis_size("near")
    level = jnp.stack([own] + [shifted(own, "far", far - i) for i in range(1, far)])
    chips = far * near
    wide = []
    for k in (-1, 0, 1, 2):
        if k:
            wide.append(shifted(level, ("far", "near"), chips - k))
        else:
            wide.append(level)
    mine = jnp.stack(wide, axis=1).reshape(chips, *own.shape)
    other = shifted(mine, "core", 1)
    core = lax.axis_index("core")
    both = jnp.stack([jnp.where(core == 0, mine, other), jnp.where(core == 0, other, mine)], axis=1)
    both = both.reshape(chips, -1, own.shape[1])
    both = jnp.concatenate([both, both], axis=0)
    at = lax.axis_index(("far", "near"))
    start = jnp.where(at == 0, 1, chips + 1 - at)
    whole = lax.dynamic_slice_in_dim(both, start, chips, axis=0)
    return whole.reshape(-1, own.shape[1])


def expert_body(rows_ref, gate_ref, up_ref, down_ref, out_ref, hidden_ref):
    inner, width = down_ref.shape
    unit, wide = 128, 256

    def hide(k, _):
        at = pl.ds(pl.multiple_of(k * unit, unit), unit)
        both = jnp.concatenate([gate_ref[:, at], up_ref[:, at]], axis=1)
        made = jnp.dot(rows_ref[...], both, preferred_element_type=jnp.float32)
        gate, upward = made[:, :unit], made[:, unit:]
        hidden = gate / (1.0 + jnp.exp(-gate)) * upward
        hidden_ref[:, at] = hidden.astype(jnp.bfloat16)

    def show(k, _):
        at = pl.ds(pl.multiple_of(k * wide, wide), wide)
        out_ref[:, at] = jnp.dot(
            hidden_ref[...], down_ref[:, at], preferred_element_type=jnp.float32
        ).astype(jnp.bfloat16)

    lax.fori_loop(0, inner // unit, hide, None)
    lax.fori_loop(0, width // wide, show, None)


def expert_part(rows_in, gate_w, up_w, down_w):
    count, width = rows_in.shape
    inner = gate_w.shape[1]
    whole = pl.BlockSpec(memory_space=pltpu.VMEM)
    return pl.pallas_call(
        expert_body,
        in_specs=[whole] * 4,
        out_specs=whole,
        out_shape=jax.ShapeDtypeStruct((count, width), jnp.bfloat16),
        scratch_shapes=[pltpu.VMEM((count, inner), jnp.bfloat16)],
        compiler_params=pltpu.CompilerParams(vmem_limit_bytes=24 << 20),
        cost_estimate=pl.CostEstimate(
            flops=6 * count * width * inner,
            bytes_accessed=6 * width * inner + 4 * count * width,
            transcendentals=count * inner,
        ),
        name="expert_part",
    )(rows_in, gate_w, up_w, down_w)


def packed(by_slot, lines):
    slots, _, width = by_slot.shape
    if slots < lines:
        part = width * slots // lines
        rest = [by_slot[s, :, part:] for s in range(slots)]
        rest = jnp.concatenate(rest, axis=1)
        rest = rest.reshape(rest.shape[0], lines - slots, part).swapaxes(0, 1)
        by_slot = jnp.concatenate([by_slot[:, :, :part], rest], axis=0)
    return jnp.transpose(by_slot, (1, 0, 2))


def unpacked(messages, slots, width):
    lines, part = messages.shape[1:]
    by_line = jnp.transpose(messages, (1, 0, 2))
    if slots == lines:
        return by_line
    rest = by_line[slots:].swapaxes(0, 1).reshape(by_line.shape[1], -1)
    tail = width - part
    return jnp.stack(
        [
            jnp.concatenate([by_line[s], rest[:, s * tail : (s + 1) * tail]], axis=1)
            for s in range(slots)
        ]
    )


def through_experts(by_slot, weights):
    slots, peers, width = by_slot.shape
    rows = by_slot.reshape(slots * peers, width)
    size = lax.axis_size("tp")
    half = rows.shape[0] // 2
    left = shifted(rows, "tp", 1)
    right = shifted(rows, "tp", size - 1)
    own = expert_part(rows, *weights)
    across = [shifted(left[:half], "tp", 1), shifted(right[half:], "tp", size - 1)]
    left, right, _ = lax.optimization_barrier((left, right, own))
    from_left = expert_part(left, *weights)
    right, _ = lax.optimization_barrier((right, from_left))
    from_right = expert_part(right, *weights)
    across, _ = lax.optimization_barrier((jnp.concatenate(across, axis=0), from_right))
    from_across = expert_part(across, *weights)
    parts = [own]
    for piece, by in ((from_left, size - 1), (from_right, 1), (from_across, 2)):
        parts.append(shifted(piece, "tp", by))
    made = sum(part.astype(jnp.float32) for part in parts).astype(jnp.bfloat16)
    return made.reshape(by_slot.shape), from_across


def shards(
    queries,
    head_key_rows,
    head_value_rows,
    input_gate_logit,
    forget_gate_preact,
    forget_log_offset,
    per_head_norm_gain,
    cell_output_matrix,
    layer_input_rows,
    expert_norm_gain,
    chosen_expert_index,
    chosen_expert_weight,
    expert_gate_matrix,
    expert_up_matrix,
    expert_down_matrix,
):
    count = queries.shape[0]
    heads = input_gate_logit.shape[0]
    queries3 = queries.reshape(count, heads, DK)
    keys3 = head_key_rows.reshape(count, heads, DK)
    values3 = head_value_rows.reshape(count, heads, DV)
    rows_at = lax.broadcasted_iota(jnp.int32, (count, count), 0)
    cols_at = lax.broadcasted_iota(jnp.int32, (count, count), 1)
    causal = cols_at <= rows_at

    log_retention = jax.nn.log_sigmoid(forget_gate_preact) + forget_log_offset
    running = jnp.dot(log_retention, (rows_at <= cols_at).astype(jnp.float32), precision=HIGHEST)
    totals = running[:, -1]
    term_log = totals[:, None] - running + input_gate_logit
    own_peak = jnp.max(term_log, axis=1)
    factors = jnp.transpose(jnp.exp(term_log - own_peak[:, None]))
    weighted = values3.astype(jnp.float32) * factors[:, :, None]
    own_memory = jnp.einsum(
        "shd,she->hde", keys3.astype(jnp.float32), weighted, precision=HIGHEST
    )

    memory_in, peak_in = states_before(own_memory, totals, own_peak)

    decay_log = jnp.where(
        causal[None],
        running[:, :, None] - running[:, None, :] + input_gate_logit[:, None, :],
        far_below,
    )
    carried_log = running + peak_in[:, None]
    peak = jnp.maximum(carried_log, jnp.max(decay_log, axis=2))
    qk_scale = DK ** (-0.5)
    scores = (
        jnp.einsum("thd,shd->hts", queries3, keys3, preferred_element_type=jnp.float32) * qk_scale
    )
    strength = scores * jnp.exp(decay_log - peak[:, :, None])
    carried = jnp.exp(carried_log - peak)
    from_memory = (
        jnp.einsum("thd,hde->the", queries3.astype(jnp.float32), memory_in, precision=HIGHEST)
        * qk_scale
    )
    within = jnp.einsum(
        "hts,she->the", strength.astype(jnp.bfloat16), values3, preferred_element_type=jnp.float32
    )
    result = within + jnp.transpose(carried)[:, :, None] * from_memory
    result = result * lax.rsqrt(jnp.mean(result * result, axis=2, keepdims=True) + norm_eps)
    result = result * per_head_norm_gain.astype(jnp.float32).reshape(heads, -1)
    mixed = result.reshape(count, -1).astype(jnp.bfloat16)

    partial_value = lax.dot_general(
        mixed,
        gathered_columns(cell_output_matrix),
        (((1,), (1,)), ((), ())),
        preferred_element_type=jnp.float32,
    ).astype(jnp.bfloat16)
    rows, width = layer_input_rows.shape
    tiles = traded(partial_value.reshape(lax.axis_size("tp"), rows, width), "tp")
    residual = layer_input_rows.astype(jnp.float32) + jnp.sum(tiles.astype(jnp.float32), axis=0)
    normed = residual * lax.rsqrt(jnp.mean(residual * residual, axis=1, keepdims=True) + norm_eps)
    normed = (normed * expert_norm_gain.astype(jnp.float32)).astype(jnp.bfloat16)

    experts = lax.axis_size(SP)
    slots = (4 * rows + experts - 1) // experts
    expert_at = jnp.arange(experts, dtype=jnp.int32)[None, :]
    named = [
        (chosen_expert_index[:, k : k + 1] == expert_at).astype(jnp.bfloat16) for k in range(2)
    ]
    below = (
        lax.broadcasted_iota(jnp.int32, (rows, rows), 1)
        < lax.broadcasted_iota(jnp.int32, (rows, rows), 0)
    ).astype(jnp.bfloat16)
    ahead = [jnp.dot(below, n, preferred_element_type=jnp.float32) for n in named]
    first = jnp.sum(named[0].astype(jnp.float32), axis=0, keepdims=True)
    ahead[1] = ahead[1] + first
    picks = []
    for k in range(2):
        place = jnp.sum(named[k].astype(jnp.float32) * ahead[k], axis=1, keepdims=True)
        slot = place.astype(jnp.int32) * experts + chosen_expert_index[:, k : k + 1]
        target = lax.broadcasted_iota(jnp.int32, (rows, experts * slots), 1)
        picks.append((slot == target).astype(jnp.bfloat16))
    outgoing = lax.dot_general(
        picks[0] + picks[1],
        normed,
        (((0,), (0,)), ((), ())),
        preferred_element_type=jnp.float32,
    ).astype(jnp.bfloat16)

    weights = (expert_gate_matrix[0], expert_up_matrix[0], expert_down_matrix[0])
    early = (slots + 1) // 2
    by_slot = outgoing.reshape(slots, experts, width)
    got_a = traded(packed(by_slot[:early], early), SP)
    got_b = traded(packed(by_slot[early:], early), SP)
    made_a, last = through_experts(unpacked(got_a, early, width), weights)
    got_b, _ = lax.optimization_barrier((got_b, last))
    back_a = traded(packed(made_a, early), SP)
    made_b, _ = through_experts(unpacked(got_b, slots - early, width), weights)
    back_b = traded(packed(made_b, early), SP)

    out = residual
    cut = early * experts
    out_a = unpacked(back_a, early, width).reshape(cut, width)
    out_b = unpacked(back_b, slots - early, width).reshape(-1, width)
    for k in range(2):
        picked = jnp.dot(picks[k][:, :cut], out_a, preferred_element_type=jnp.float32)
        out = out + chosen_expert_weight[:, k : k + 1] * picked
    for k in range(2):
        picked = jnp.dot(picks[k][:, cut:], out_b, preferred_element_type=jnp.float32)
        out = out + chosen_expert_weight[:, k : k + 1] * picked
    return out.astype(jnp.bfloat16)


def solution(mesh):
    sp = mesh.shape["sp"]
    torus = Mesh(
        mesh.devices.reshape(mesh.shape["grp"], sp // 8, 4, 2, mesh.shape["tp"]), GRP_SP_TP
    )
    return jax.shard_map(
        shards,
        mesh=torus,
        in_specs=(
            P(GRP_SP, "tp"),
            P(GRP_SP, "tp"),
            P(GRP_SP, "tp"),
            P("tp", GRP_SP),
            P("tp", GRP_SP),
            P("tp", GRP_SP),
            P("tp"),
            P("tp", SP),
            P(GRP_SP_TP, None),
            P(),
            P(GRP_SP_TP, None),
            P(GRP_SP_TP, None),
            P(SP, None, "tp"),
            P(SP, None, "tp"),
            P(SP, "tp", None),
        ),
        out_specs=P(GRP_SP_TP, None),
        check_vma=False,
    )
```

```python
import jax
import jax.numpy as jnp
from jax import lax
from jax.experimental import pallas as pl
from jax.experimental.pallas import tpu as pltpu
from jax.sharding import Mesh
from jax.sharding import PartitionSpec as P


DK = 64
DV = 128
NEAR = ("near", "core")
SP = ("far", *NEAR)
GRP_SP = ("grp", *SP)
GRP_SP_TP = (*GRP_SP, "tp")

far_below = -1e30
norm_eps = 1e-06
HIGHEST = lax.Precision.HIGHEST


def shifted(x, axis, by):
    size = lax.axis_size(axis)
    return lax.ppermute(x, axis, [(i, (i + by) % size) for i in range(size)])


def traded(x, axis):
    return lax.all_to_all(x, axis, split_axis=0, concat_axis=0, tiled=True)


def strength_of(totals, peaks):
    size = totals.shape[0]
    shape = (size + 1, size, size)
    t, s, u = (lax.broadcasted_iota(jnp.int32, shape, d) for d in range(3))
    decay = jnp.sum(jnp.where((s < u) & (u < t), totals[None, None, :], 0.0), axis=2)
    earlier = s[:, :, 0] < t[:, :, 0]
    logs = jnp.where(earlier, decay + peaks[None, :], far_below)
    tops = jnp.max(logs, axis=1)
    return jnp.where(earlier, jnp.exp(logs - tops[:, None]), 0.0), tops


def with_header(body, *scalars):
    count, _, lanes = body.shape
    lines = [jnp.broadcast_to(x.reshape(count, 1, 1), (count, 1, lanes)) for x in scalars]
    lines.append(jnp.zeros((count, 8 - len(scalars), lanes), jnp.float32))
    return jnp.concatenate([body, *lines], axis=1)


def states_before(memory, totals, peaks):
    heads, dk, dv = memory.shape
    near = lax.axis_size(NEAR)
    far = lax.axis_size("far")
    rows = heads * dk // near
    per_head = near // heads
    sent = with_header(
        memory.reshape(near, rows, dv), jnp.repeat(totals, per_head), jnp.repeat(peaks, per_head)
    )
    got = traded(sent, NEAR)
    parts, total, peak = got[:, :rows], got[:, rows, 0], got[:, rows + 1, 0]
    size = total.shape[0]
    weight, tops = strength_of(total, peak)
    whole = jnp.sum(weight[size][:, None, None] * parts, axis=0)
    whole = with_header(whole[None], jnp.sum(total).reshape(1), tops[size].reshape(1))[0]
    group = lax.axis_index("far")
    before = []
    for back in range(far - 1, 0, -1):
        other = lax.ppermute(whole, "far", [(i, i + back) for i in range(far - back)])
        before.append(jnp.where(group >= back, other, jnp.zeros_like(other)))
    stack = jnp.stack(before)
    known = group >= jnp.arange(far - 1, 0, -1)
    all_total = jnp.concatenate([stack[:, rows, 0], total])
    all_peak = jnp.concatenate([jnp.where(known, stack[:, rows + 1, 0], far_below), peak])
    weight, tops = strength_of(all_total, all_peak)
    weight, tops = weight[far - 1 : -1], tops[far - 1 : -1]
    states = jnp.concatenate([stack[:, :rows], parts], axis=0)
    states = jnp.sum(weight[:, :, None, None] * states[None], axis=1)
    mine = traded(with_header(states, tops), NEAR)
    return mine[:, :rows].reshape(heads, dk, dv), mine[::per_head, rows, 0]


def gathered_columns(matrix):
    own = jnp.transpose(matrix)
    far, near = lax.axis_size("far"), lax.axis_size("near")
    level = jnp.stack([own] + [shifted(own, "far", far - i) for i in range(1, far)])
    chips = far * near
    wide = []
    for k in (-1, 0, 1, 2):
        if k:
            wide.append(shifted(level, ("far", "near"), chips - k))
        else:
            wide.append(level)
    mine = jnp.stack(wide, axis=1).reshape(chips, *own.shape)
    other = shifted(mine, "core", 1)
    core = lax.axis_index("core")
    both = jnp.stack([jnp.where(core == 0, mine, other), jnp.where(core == 0, other, mine)], axis=1)
    both = both.reshape(chips, -1, own.shape[1])
    both = jnp.concatenate([both, both], axis=0)
    at = lax.axis_index(("far", "near"))
    start = jnp.where(at == 0, 1, chips + 1 - at)
    whole = lax.dynamic_slice_in_dim(both, start, chips, axis=0)
    return whole.reshape(-1, own.shape[1])


UNIT = 128
WIDE = 256


def expert_body(
    one_ref, two_ref, gate_hbm, up_hbm, down_hbm, one_out, two_out,
    gate_ref, up_ref, down_ref, hidden_ref, gate_sem, up_sem, down_sem,
):
    units, columns, count = gate_ref.shape[0], down_ref.shape[0], one_ref.shape[0]

    def block(k, size):
        return pl.ds(pl.multiple_of(k * size, size), size)

    def gate_copy(k):
        return pltpu.make_async_copy(gate_hbm.at[:, block(k, UNIT)], gate_ref.at[k], gate_sem.at[k])

    def up_copy(k):
        return pltpu.make_async_copy(up_hbm.at[:, block(k, UNIT)], up_ref.at[k], up_sem.at[k])

    def down_copy(k):
        return pltpu.make_async_copy(down_hbm.at[:, block(k, WIDE)], down_ref.at[k], down_sem.at[k])

    def ask(k, _):
        gate_copy(k).start()
        up_copy(k).start()

    def hide(k, _):
        gate_copy(k).wait()
        up_copy(k).wait()
        both = jnp.concatenate([gate_ref[k], up_ref[k]], axis=1)
        rows = jnp.concatenate([one_ref[...], two_ref[...]], axis=0)
        made = jnp.dot(rows, both, preferred_element_type=jnp.float32)
        gate, upward = made[:, :UNIT], made[:, UNIT:]
        hidden = gate / (1.0 + jnp.exp(-gate)) * upward
        hidden_ref[:, block(k, UNIT)] = hidden.astype(jnp.bfloat16)

    def show(k, _):
        down_copy(k).wait()
        made = jnp.dot(hidden_ref[...], down_ref[k], preferred_element_type=jnp.float32)
        made = made.astype(jnp.bfloat16)
        one_out[:, block(k, WIDE)] = made[:count]
        two_out[:, block(k, WIDE)] = made[count:]

    lax.fori_loop(0, units, ask, None)
    lax.fori_loop(0, columns, lambda k, _: down_copy(k).start(), None)
    lax.fori_loop(0, units, hide, None)
    lax.fori_loop(0, columns, show, None)


def expert_parts(one, two, gate_w, up_w, down_w):
    count, width = one.shape
    inner = gate_w.shape[1]
    units, columns = inner // UNIT, width // WIDE
    whole = pl.BlockSpec(memory_space=pltpu.VMEM)
    stored = pl.BlockSpec(memory_space=pltpu.HBM)
    rows = jax.ShapeDtypeStruct((count, width), jnp.bfloat16)
    return pl.pallas_call(
        expert_body,
        in_specs=[whole, whole, stored, stored, stored],
        out_specs=[whole, whole],
        out_shape=[rows, rows],
        scratch_shapes=[
            pltpu.VMEM((units, width, UNIT), jnp.bfloat16),
            pltpu.VMEM((units, width, UNIT), jnp.bfloat16),
            pltpu.VMEM((columns, inner, WIDE), jnp.bfloat16),
            pltpu.VMEM((2 * count, inner), jnp.bfloat16),
            pltpu.SemaphoreType.DMA((units,)),
            pltpu.SemaphoreType.DMA((units,)),
            pltpu.SemaphoreType.DMA((columns,)),
        ],
        compiler_params=pltpu.CompilerParams(vmem_limit_bytes=32 << 20),
        cost_estimate=pl.CostEstimate(
            flops=12 * count * width * inner,
            bytes_accessed=6 * width * inner + 8 * count * width,
            transcendentals=2 * count * inner,
        ),
        name="expert_parts",
    )(one, two, gate_w, up_w, down_w)


def packed(by_slot, lines):
    slots, _, width = by_slot.shape
    if slots < lines:
        part = width * slots // lines
        rest = [by_slot[s, :, part:] for s in range(slots)]
        rest = jnp.concatenate(rest, axis=1)
        rest = rest.reshape(rest.shape[0], lines - slots, part).swapaxes(0, 1)
        by_slot = jnp.concatenate([by_slot[:, :, :part], rest], axis=0)
    return jnp.transpose(by_slot, (1, 0, 2))


def unpacked(messages, slots, width):
    lines, part = messages.shape[1:]
    by_line = jnp.transpose(messages, (1, 0, 2))
    if slots == lines:
        return by_line
    rest = by_line[slots:].swapaxes(0, 1).reshape(by_line.shape[1], -1)
    tail = width - part
    return jnp.stack(
        [
            jnp.concatenate([by_line[s], rest[:, s * tail : (s + 1) * tail]], axis=1)
            for s in range(slots)
        ]
    )


def through_experts(by_slot, weights):
    slots, peers, width = by_slot.shape
    rows = by_slot.reshape(slots * peers, width)
    size = lax.axis_size("tp")
    half = rows.shape[0] // 2
    left = shifted(rows, "tp", 1)
    right = shifted(rows, "tp", size - 1)
    across = [shifted(left[:half], "tp", 1), shifted(right[half:], "tp", size - 1)]
    left, right = lax.optimization_barrier((left, right))
    from_left, from_right = expert_parts(left, right, *weights)
    parts = [shifted(from_left, "tp", size - 1), shifted(from_right, "tp", 1)]
    across, rows, _ = lax.optimization_barrier((jnp.concatenate(across, axis=0), rows, from_right))
    from_across, own = expert_parts(across, rows, *weights)
    parts = [own, *parts, shifted(from_across, "tp", 2)]
    made = sum(part.astype(jnp.float32) for part in parts).astype(jnp.bfloat16)
    return made.reshape(by_slot.shape), from_across


def shards(
    queries,
    head_key_rows,
    head_value_rows,
    input_gate_logit,
    forget_gate_preact,
    forget_log_offset,
    per_head_norm_gain,
    cell_output_matrix,
    layer_input_rows,
    expert_norm_gain,
    chosen_expert_index,
    chosen_expert_weight,
    expert_gate_matrix,
    expert_up_matrix,
    expert_down_matrix,
):
    count = queries.shape[0]
    heads = input_gate_logit.shape[0]
    queries3 = queries.reshape(count, heads, DK)
    keys3 = head_key_rows.reshape(count, heads, DK)
    values3 = head_value_rows.reshape(count, heads, DV)
    rows_at = lax.broadcasted_iota(jnp.int32, (count, count), 0)
    cols_at = lax.broadcasted_iota(jnp.int32, (count, count), 1)
    causal = cols_at <= rows_at

    log_retention = jax.nn.log_sigmoid(forget_gate_preact) + forget_log_offset
    running = jnp.dot(log_retention, (rows_at <= cols_at).astype(jnp.float32), precision=HIGHEST)
    totals = running[:, -1]
    term_log = totals[:, None] - running + input_gate_logit
    own_peak = jnp.max(term_log, axis=1)
    factors = jnp.transpose(jnp.exp(term_log - own_peak[:, None]))
    weighted = values3.astype(jnp.float32) * factors[:, :, None]
    own_memory = jnp.einsum(
        "shd,she->hde", keys3.astype(jnp.float32), weighted, precision=HIGHEST
    )

    memory_in, peak_in = states_before(own_memory, totals, own_peak)

    decay_log = jnp.where(
        causal[None],
        running[:, :, None] - running[:, None, :] + input_gate_logit[:, None, :],
        far_below,
    )
    carried_log = running + peak_in[:, None]
    peak = jnp.maximum(carried_log, jnp.max(decay_log, axis=2))
    qk_scale = DK ** (-0.5)
    scores = (
        jnp.einsum("thd,shd->hts", queries3, keys3, preferred_element_type=jnp.float32) * qk_scale
    )
    strength = scores * jnp.exp(decay_log - peak[:, :, None])
    carried = jnp.exp(carried_log - peak)
    from_memory = (
        jnp.einsum("thd,hde->the", queries3.astype(jnp.float32), memory_in, precision=HIGHEST)
        * qk_scale
    )
    within = jnp.einsum(
        "hts,she->the", strength.astype(jnp.bfloat16), values3, preferred_element_type=jnp.float32
    )
    result = within + jnp.transpose(carried)[:, :, None] * from_memory
    result = result * lax.rsqrt(jnp.mean(result * result, axis=2, keepdims=True) + norm_eps)
    result = result * per_head_norm_gain.astype(jnp.float32).reshape(heads, -1)
    mixed = result.reshape(count, -1).astype(jnp.bfloat16)

    partial_value = lax.dot_general(
        mixed,
        gathered_columns(cell_output_matrix),
        (((1,), (1,)), ((), ())),
        preferred_element_type=jnp.float32,
    ).astype(jnp.bfloat16)
    rows, width = layer_input_rows.shape
    tiles = traded(partial_value.reshape(lax.axis_size("tp"), rows, width), "tp")
    residual = layer_input_rows.astype(jnp.float32) + jnp.sum(tiles.astype(jnp.float32), axis=0)
    normed = residual * lax.rsqrt(jnp.mean(residual * residual, axis=1, keepdims=True) + norm_eps)
    normed = (normed * expert_norm_gain.astype(jnp.float32)).astype(jnp.bfloat16)

    experts = lax.axis_size(SP)
    slots = (4 * rows + experts - 1) // experts
    expert_at = jnp.arange(experts, dtype=jnp.int32)[None, :]
    named = [
        (chosen_expert_index[:, k : k + 1] == expert_at).astype(jnp.bfloat16) for k in range(2)
    ]
    below = (
        lax.broadcasted_iota(jnp.int32, (rows, rows), 1)
        < lax.broadcasted_iota(jnp.int32, (rows, rows), 0)
    ).astype(jnp.bfloat16)
    ahead = [jnp.dot(below, n, preferred_element_type=jnp.float32) for n in named]
    first = jnp.sum(named[0].astype(jnp.float32), axis=0, keepdims=True)
    ahead[1] = ahead[1] + first
    picks = []
    for k in range(2):
        place = jnp.sum(named[k].astype(jnp.float32) * ahead[k], axis=1, keepdims=True)
        slot = place.astype(jnp.int32) * experts + chosen_expert_index[:, k : k + 1]
        target = lax.broadcasted_iota(jnp.int32, (rows, experts * slots), 1)
        picks.append((slot == target).astype(jnp.bfloat16))
    outgoing = lax.dot_general(
        picks[0] + picks[1],
        normed,
        (((0,), (0,)), ((), ())),
        preferred_element_type=jnp.float32,
    ).astype(jnp.bfloat16)

    weights = tuple(pltpu.with_memory_space_constraint(w[0], pltpu.HBM) for w in (expert_gate_matrix, expert_up_matrix, expert_down_matrix))
    early = (slots + 1) // 2
    by_slot = outgoing.reshape(slots, experts, width)
    got_a = traded(packed(by_slot[:early], early), SP)
    got_b = traded(packed(by_slot[early:], early), SP)
    made_a, last = through_experts(unpacked(got_a, early, width), weights)
    got_b, _ = lax.optimization_barrier((got_b, last))
    back_a = traded(packed(made_a, early), SP)
    made_b, _ = through_experts(unpacked(got_b, slots - early, width), weights)
    back_b = traded(packed(made_b, early), SP)

    out = residual
    cut = early * experts
    out_a = unpacked(back_a, early, width).reshape(cut, width)
    out_b = unpacked(back_b, slots - early, width).reshape(-1, width)
    for k in range(2):
        picked = jnp.dot(picks[k][:, :cut], out_a, preferred_element_type=jnp.float32)
        out = out + chosen_expert_weight[:, k : k + 1] * picked
    for k in range(2):
        picked = jnp.dot(picks[k][:, cut:], out_b, preferred_element_type=jnp.float32)
        out = out + chosen_expert_weight[:, k : k + 1] * picked
    return out.astype(jnp.bfloat16)


def solution(mesh):
    sp = mesh.shape["sp"]
    torus = Mesh(
        mesh.devices.reshape(mesh.shape["grp"], sp // 8, 4, 2, mesh.shape["tp"]), GRP_SP_TP
    )
    return jax.shard_map(
        shards,
        mesh=torus,
        in_specs=(
            P(GRP_SP, "tp"),
            P(GRP_SP, "tp"),
            P(GRP_SP, "tp"),
            P("tp", GRP_SP),
            P("tp", GRP_SP),
            P("tp", GRP_SP),
            P("tp"),
            P("tp", SP),
            P(GRP_SP_TP, None),
            P(),
            P(GRP_SP_TP, None),
            P(GRP_SP_TP, None),
            P(SP, None, "tp"),
            P(SP, None, "tp"),
            P(SP, "tp", None),
        ),
        out_specs=P(GRP_SP_TP, None),
        check_vma=False,
    )
```

```python
import jax
import jax.numpy as jnp
from jax import lax
from jax.experimental import pallas as pl
from jax.experimental.pallas import tpu as pltpu
from jax.sharding import Mesh
from jax.sharding import PartitionSpec as P


DK = 64
DV = 128
NEAR = ("near", "core")
SP = ("far", *NEAR)
GRP_SP = ("grp", *SP)
GRP_SP_TP = (*GRP_SP, "tp")

far_below = -1e30
norm_eps = 1e-06
HIGHEST = lax.Precision.HIGHEST


def shifted(x, axis, by):
    size = lax.axis_size(axis)
    return lax.ppermute(x, axis, [(i, (i + by) % size) for i in range(size)])


def traded(x, axis):
    return lax.all_to_all(x, axis, split_axis=0, concat_axis=0, tiled=True)


def combined(state, total, part, peak):
    memory, top = state
    kept = top + total
    higher = jnp.maximum(kept, peak)
    return jnp.exp(kept - higher) * memory + jnp.exp(peak - higher) * part, higher


def group_body(parts_ref, out_ref):
    size, lines, lanes = parts_ref.shape
    rows = lines - 8
    state = parts_ref[0, :rows], parts_ref[0, rows + 1 : rows + 2]
    total = parts_ref[0, rows : rows + 1]
    for p in range(1, size):
        more = parts_ref[p, rows : rows + 1]
        state = combined(state, more, parts_ref[p, :rows], parts_ref[p, rows + 1 : rows + 2])
        total = total + more
    out_ref[:rows] = state[0]
    line = lax.broadcasted_iota(jnp.int32, (8, lanes), 0)
    out_ref[rows:] = jnp.where(line == 0, total, state[1])


def before_body(group_ref, parts_ref, *refs):
    *others, out_ref = refs
    size, lines, lanes = parts_ref.shape
    rows = lines - 8
    state = jnp.zeros((rows, lanes), jnp.float32), jnp.full((1, lanes), far_below, jnp.float32)
    for back, other in zip(range(len(others), 0, -1), others):
        known = group_ref[0] >= back
        total = jnp.where(known, other[rows : rows + 1], 0.0)
        peak = jnp.where(known, other[rows + 1 : rows + 2], far_below)
        state = combined(state, total, jnp.where(known, other[:rows], 0.0), peak)
    for p in range(size):
        out_ref[p, :rows] = state[0]
        out_ref[p, rows:] = jnp.broadcast_to(state[1], (8, lanes))
        total, peak = parts_ref[p, rows : rows + 1], parts_ref[p, rows + 1 : rows + 2]
        state = combined(state, total, parts_ref[p, :rows], peak)


def with_header(body, *scalars):
    count, _, lanes = body.shape
    lines = [jnp.broadcast_to(x.reshape(count, 1, 1), (count, 1, lanes)) for x in scalars]
    lines.append(jnp.zeros((count, 8 - len(scalars), lanes), jnp.float32))
    return jnp.concatenate([body, *lines], axis=1)


def states_before(memory, totals, peaks):
    heads, dk, dv = memory.shape
    near = lax.axis_size(NEAR)
    far = lax.axis_size("far")
    rows = heads * dk // near
    per_head = near // heads
    sent = with_header(
        memory.reshape(near, rows, dv), jnp.repeat(totals, per_head), jnp.repeat(peaks, per_head)
    )
    got = traded(sent, NEAR)
    whole = pl.pallas_call(
        group_body,
        out_shape=jax.ShapeDtypeStruct(got.shape[1:], jnp.float32),
        compiler_params=pltpu.CompilerParams(vmem_limit_bytes=4 << 20),
        name="group_state",
    )(got)
    before = []
    for back in range(far - 1, 0, -1):
        before.append(lax.ppermute(whole, "far", [(i, i + back) for i in range(far - back)]))
    whole_spec = pl.BlockSpec(memory_space=pltpu.VMEM)
    states = pl.pallas_call(
        before_body,
        in_specs=[pl.BlockSpec(memory_space=pltpu.SMEM)] + [whole_spec] * far,
        out_specs=whole_spec,
        out_shape=jax.ShapeDtypeStruct(got.shape, jnp.float32),
        compiler_params=pltpu.CompilerParams(vmem_limit_bytes=4 << 20),
        name="states_before",
    )(lax.axis_index("far").reshape(1), got, *before)
    mine = traded(states, NEAR)
    return mine[:, :rows].reshape(heads, dk, dv), mine[::per_head, rows, 0]


def gathered_columns(matrix):
    own = jnp.transpose(matrix)
    far, near = lax.axis_size("far"), lax.axis_size("near")
    level = jnp.stack([own] + [shifted(own, "far", far - i) for i in range(1, far)])
    chips = far * near
    wide = []
    for k in (-1, 0, 1, 2):
        if k:
            wide.append(shifted(level, ("far", "near"), chips - k))
        else:
            wide.append(level)
    mine = jnp.stack(wide, axis=1).reshape(chips, *own.shape)
    other = shifted(mine, "core", 1)
    core = lax.axis_index("core")
    both = jnp.stack([jnp.where(core == 0, mine, other), jnp.where(core == 0, other, mine)], axis=1)
    both = both.reshape(chips, -1, own.shape[1])
    both = jnp.concatenate([both, both], axis=0)
    at = lax.axis_index(("far", "near"))
    start = jnp.where(at == 0, 1, chips + 1 - at)
    whole = lax.dynamic_slice_in_dim(both, start, chips, axis=0)
    return whole.reshape(-1, own.shape[1])


UNIT = 128
WIDE = 256


def expert_body(
    one_ref, two_ref, gate_hbm, up_hbm, down_hbm, one_out, two_out,
    gate_ref, up_ref, down_ref, hidden_ref, gate_sem, up_sem, down_sem,
):
    units, columns, count = gate_ref.shape[0], down_ref.shape[0], one_ref.shape[0]

    def block(k, size):
        return pl.ds(pl.multiple_of(k * size, size), size)

    def gate_copy(k):
        return pltpu.make_async_copy(gate_hbm.at[:, block(k, UNIT)], gate_ref.at[k], gate_sem.at[k])

    def up_copy(k):
        return pltpu.make_async_copy(up_hbm.at[:, block(k, UNIT)], up_ref.at[k], up_sem.at[k])

    def down_copy(k):
        return pltpu.make_async_copy(down_hbm.at[:, block(k, WIDE)], down_ref.at[k], down_sem.at[k])

    def ask(k, _):
        gate_copy(k).start()
        up_copy(k).start()

    def hide(k, _):
        gate_copy(k).wait()
        up_copy(k).wait()
        both = jnp.concatenate([gate_ref[k], up_ref[k]], axis=1)
        rows = jnp.concatenate([one_ref[...], two_ref[...]], axis=0)
        made = jnp.dot(rows, both, preferred_element_type=jnp.float32)
        gate, upward = made[:, :UNIT], made[:, UNIT:]
        hidden = gate / (1.0 + jnp.exp(-gate)) * upward
        hidden_ref[:, block(k, UNIT)] = hidden.astype(jnp.bfloat16)

    def show(k, _):
        down_copy(k).wait()
        made = jnp.dot(hidden_ref[...], down_ref[k], preferred_element_type=jnp.float32)
        made = made.astype(jnp.bfloat16)
        one_out[:, block(k, WIDE)] = made[:count]
        two_out[:, block(k, WIDE)] = made[count:]

    lax.fori_loop(0, units, ask, None)
    lax.fori_loop(0, columns, lambda k, _: down_copy(k).start(), None)
    lax.fori_loop(0, units, hide, None)
    lax.fori_loop(0, columns, show, None)


def expert_parts(one, two, gate_w, up_w, down_w):
    count, width = one.shape
    inner = gate_w.shape[1]
    units, columns = inner // UNIT, width // WIDE
    whole = pl.BlockSpec(memory_space=pltpu.VMEM)
    stored = pl.BlockSpec(memory_space=pltpu.HBM)
    rows = jax.ShapeDtypeStruct((count, width), jnp.bfloat16)
    return pl.pallas_call(
        expert_body,
        in_specs=[whole, whole, stored, stored, stored],
        out_specs=[whole, whole],
        out_shape=[rows, rows],
        scratch_shapes=[
            pltpu.VMEM((units, width, UNIT), jnp.bfloat16),
            pltpu.VMEM((units, width, UNIT), jnp.bfloat16),
            pltpu.VMEM((columns, inner, WIDE), jnp.bfloat16),
            pltpu.VMEM((2 * count, inner), jnp.bfloat16),
            pltpu.SemaphoreType.DMA((units,)),
            pltpu.SemaphoreType.DMA((units,)),
            pltpu.SemaphoreType.DMA((columns,)),
        ],
        compiler_params=pltpu.CompilerParams(vmem_limit_bytes=32 << 20),
        cost_estimate=pl.CostEstimate(
            flops=12 * count * width * inner,
            bytes_accessed=6 * width * inner + 8 * count * width,
            transcendentals=2 * count * inner,
        ),
        name="expert_parts",
    )(one, two, gate_w, up_w, down_w)


def packed(by_slot, lines):
    slots, _, width = by_slot.shape
    if slots < lines:
        part = width * slots // lines
        rest = [by_slot[s, :, part:] for s in range(slots)]
        rest = jnp.concatenate(rest, axis=1)
        rest = rest.reshape(rest.shape[0], lines - slots, part).swapaxes(0, 1)
        by_slot = jnp.concatenate([by_slot[:, :, :part], rest], axis=0)
    return jnp.transpose(by_slot, (1, 0, 2))


def unpacked(messages, slots, width):
    lines, part = messages.shape[1:]
    by_line = jnp.transpose(messages, (1, 0, 2))
    if slots == lines:
        return by_line
    rest = by_line[slots:].swapaxes(0, 1).reshape(by_line.shape[1], -1)
    tail = width - part
    return jnp.stack(
        [
            jnp.concatenate([by_line[s], rest[:, s * tail : (s + 1) * tail]], axis=1)
            for s in range(slots)
        ]
    )


def through_experts(by_slot, weights):
    slots, peers, width = by_slot.shape
    rows = by_slot.reshape(slots * peers, width)
    size = lax.axis_size("tp")
    half = rows.shape[0] // 2
    left = shifted(rows, "tp", 1)
    right = shifted(rows, "tp", size - 1)
    across = [shifted(left[:half], "tp", 1), shifted(right[half:], "tp", size - 1)]
    left, right = lax.optimization_barrier((left, right))
    from_left, from_right = expert_parts(left, right, *weights)
    parts = [shifted(from_left, "tp", size - 1), shifted(from_right, "tp", 1)]
    across, rows, _ = lax.optimization_barrier((jnp.concatenate(across, axis=0), rows, from_right))
    from_across, own = expert_parts(across, rows, *weights)
    parts = [own, *parts, shifted(from_across, "tp", 2)]
    made = sum(part.astype(jnp.float32) for part in parts).astype(jnp.bfloat16)
    return made.reshape(by_slot.shape), from_across


def shards(
    queries,
    head_key_rows,
    head_value_rows,
    input_gate_logit,
    forget_gate_preact,
    forget_log_offset,
    per_head_norm_gain,
    cell_output_matrix,
    layer_input_rows,
    expert_norm_gain,
    chosen_expert_index,
    chosen_expert_weight,
    expert_gate_matrix,
    expert_up_matrix,
    expert_down_matrix,
):
    count = queries.shape[0]
    heads = input_gate_logit.shape[0]
    queries3 = queries.reshape(count, heads, DK)
    keys3 = head_key_rows.reshape(count, heads, DK)
    values3 = head_value_rows.reshape(count, heads, DV)
    rows_at = lax.broadcasted_iota(jnp.int32, (count, count), 0)
    cols_at = lax.broadcasted_iota(jnp.int32, (count, count), 1)
    causal = cols_at <= rows_at

    log_retention = jax.nn.log_sigmoid(forget_gate_preact) + forget_log_offset
    running = jnp.dot(log_retention, (rows_at <= cols_at).astype(jnp.float32), precision=HIGHEST)
    totals = running[:, -1]
    term_log = totals[:, None] - running + input_gate_logit
    own_peak = jnp.max(term_log, axis=1)
    factors = jnp.transpose(jnp.exp(term_log - own_peak[:, None]))
    weighted = values3.astype(jnp.float32) * factors[:, :, None]
    own_memory = jnp.einsum(
        "shd,she->hde", keys3.astype(jnp.float32), weighted, precision=HIGHEST
    )

    memory_in, peak_in = states_before(own_memory, totals, own_peak)

    decay_log = jnp.where(
        causal[None],
        running[:, :, None] - running[:, None, :] + input_gate_logit[:, None, :],
        far_below,
    )
    carried_log = running + peak_in[:, None]
    peak = jnp.maximum(carried_log, jnp.max(decay_log, axis=2))
    qk_scale = DK ** (-0.5)
    scores = (
        jnp.einsum("thd,shd->hts", queries3, keys3, preferred_element_type=jnp.float32) * qk_scale
    )
    strength = scores * jnp.exp(decay_log - peak[:, :, None])
    carried = jnp.exp(carried_log - peak)
    from_memory = (
        jnp.einsum("thd,hde->the", queries3.astype(jnp.float32), memory_in, precision=HIGHEST)
        * qk_scale
    )
    within = jnp.einsum(
        "hts,she->the", strength.astype(jnp.bfloat16), values3, preferred_element_type=jnp.float32
    )
    result = within + jnp.transpose(carried)[:, :, None] * from_memory
    result = result * lax.rsqrt(jnp.mean(result * result, axis=2, keepdims=True) + norm_eps)
    result = result * per_head_norm_gain.astype(jnp.float32).reshape(heads, -1)
    mixed = result.reshape(count, -1).astype(jnp.bfloat16)

    partial_value = lax.dot_general(
        mixed,
        gathered_columns(cell_output_matrix),
        (((1,), (1,)), ((), ())),
        preferred_element_type=jnp.float32,
    ).astype(jnp.bfloat16)
    rows, width = layer_input_rows.shape
    tiles = traded(partial_value.reshape(lax.axis_size("tp"), rows, width), "tp")
    residual = layer_input_rows.astype(jnp.float32) + jnp.sum(tiles.astype(jnp.float32), axis=0)
    normed = residual * lax.rsqrt(jnp.mean(residual * residual, axis=1, keepdims=True) + norm_eps)
    normed = (normed * expert_norm_gain.astype(jnp.float32)).astype(jnp.bfloat16)

    experts = lax.axis_size(SP)
    slots = (4 * rows + experts - 1) // experts
    expert_at = jnp.arange(experts, dtype=jnp.int32)[None, :]
    named = [
        (chosen_expert_index[:, k : k + 1] == expert_at).astype(jnp.bfloat16) for k in range(2)
    ]
    below = (
        lax.broadcasted_iota(jnp.int32, (rows, rows), 1)
        < lax.broadcasted_iota(jnp.int32, (rows, rows), 0)
    ).astype(jnp.bfloat16)
    ahead = [jnp.dot(below, n, preferred_element_type=jnp.float32) for n in named]
    first = jnp.sum(named[0].astype(jnp.float32), axis=0, keepdims=True)
    ahead[1] = ahead[1] + first
    picks = []
    for k in range(2):
        place = jnp.sum(named[k].astype(jnp.float32) * ahead[k], axis=1, keepdims=True)
        slot = place.astype(jnp.int32) * experts + chosen_expert_index[:, k : k + 1]
        target = lax.broadcasted_iota(jnp.int32, (rows, experts * slots), 1)
        picks.append((slot == target).astype(jnp.bfloat16))
    outgoing = lax.dot_general(
        picks[0] + picks[1],
        normed,
        (((0,), (0,)), ((), ())),
        preferred_element_type=jnp.float32,
    ).astype(jnp.bfloat16)

    weights = tuple(pltpu.with_memory_space_constraint(w[0], pltpu.HBM) for w in (expert_gate_matrix, expert_up_matrix, expert_down_matrix))
    early, lines = slots // 2, (slots + 1) // 2
    by_slot = outgoing.reshape(slots, experts, width)
    got_a = traded(packed(by_slot[:early], lines), SP)
    got_b = traded(packed(by_slot[early:], lines), SP)
    made_a, last = through_experts(unpacked(got_a, early, width), weights)
    got_b, _ = lax.optimization_barrier((got_b, last))
    back_a = traded(packed(made_a, lines), SP)
    made_b, _ = through_experts(unpacked(got_b, slots - early, width), weights)
    back_b = traded(packed(made_b, lines), SP)

    out = residual
    cut = early * experts
    out_a = unpacked(back_a, early, width).reshape(cut, width)
    out_b = unpacked(back_b, slots - early, width).reshape(-1, width)
    for k in range(2):
        picked = jnp.dot(picks[k][:, :cut], out_a, preferred_element_type=jnp.float32)
        out = out + chosen_expert_weight[:, k : k + 1] * picked
    for k in range(2):
        picked = jnp.dot(picks[k][:, cut:], out_b, preferred_element_type=jnp.float32)
        out = out + chosen_expert_weight[:, k : k + 1] * picked
    return out.astype(jnp.bfloat16)


def solution(mesh):
    sp = mesh.shape["sp"]
    torus = Mesh(
        mesh.devices.reshape(mesh.shape["grp"], sp // 8, 4, 2, mesh.shape["tp"]), GRP_SP_TP
    )
    return jax.shard_map(
        shards,
        mesh=torus,
        in_specs=(
            P(GRP_SP, "tp"),
            P(GRP_SP, "tp"),
            P(GRP_SP, "tp"),
            P("tp", GRP_SP),
            P("tp", GRP_SP),
            P("tp", GRP_SP),
            P("tp"),
            P("tp", SP),
            P(GRP_SP_TP, None),
            P(),
            P(GRP_SP_TP, None),
            P(GRP_SP_TP, None),
            P(SP, None, "tp"),
            P(SP, None, "tp"),
            P(SP, "tp", None),
        ),
        out_specs=P(GRP_SP_TP, None),
        check_vma=False,
    )
```

```python
import jax
import jax.numpy as jnp
from jax import lax
from jax.experimental import pallas as pl
from jax.experimental.pallas import tpu as pltpu
from jax.sharding import Mesh
from jax.sharding import PartitionSpec as P


DK = 64
DV = 128
NEAR = ("near", "core")
SP = ("far", *NEAR)
GRP_SP = ("grp", *SP)
GRP_SP_TP = (*GRP_SP, "tp")

far_below = -1e30
norm_eps = 1e-06
HIGHEST = lax.Precision.HIGHEST


def shifted(x, axis, by):
    size = lax.axis_size(axis)
    return lax.ppermute(x, axis, [(i, (i + by) % size) for i in range(size)])


def traded(x, axis):
    return lax.all_to_all(x, axis, split_axis=0, concat_axis=0, tiled=True)


def combined(state, total, part, peak):
    memory, top = state
    kept = top + total
    higher = jnp.maximum(kept, peak)
    return jnp.exp(kept - higher) * memory + jnp.exp(peak - higher) * part, higher


def group_body(parts_ref, out_ref):
    size, lines, lanes = parts_ref.shape
    rows = lines - 8
    state = parts_ref[0, :rows], parts_ref[0, rows + 1 : rows + 2]
    total = parts_ref[0, rows : rows + 1]
    for p in range(1, size):
        more = parts_ref[p, rows : rows + 1]
        state = combined(state, more, parts_ref[p, :rows], parts_ref[p, rows + 1 : rows + 2])
        total = total + more
    out_ref[:rows] = state[0]
    line = lax.broadcasted_iota(jnp.int32, (8, lanes), 0)
    out_ref[rows:] = jnp.where(line == 0, total, state[1])


def before_body(group_ref, parts_ref, *refs):
    *others, out_ref = refs
    size, lines, lanes = parts_ref.shape
    rows = lines - 8
    state = jnp.zeros((rows, lanes), jnp.float32), jnp.full((1, lanes), far_below, jnp.float32)
    for back, other in zip(range(len(others), 0, -1), others):
        known = group_ref[0] >= back
        total = jnp.where(known, other[rows : rows + 1], 0.0)
        peak = jnp.where(known, other[rows + 1 : rows + 2], far_below)
        state = combined(state, total, jnp.where(known, other[:rows], 0.0), peak)
    for p in range(size):
        out_ref[p, :rows] = state[0]
        out_ref[p, rows:] = jnp.broadcast_to(state[1], (8, lanes))
        total, peak = parts_ref[p, rows : rows + 1], parts_ref[p, rows + 1 : rows + 2]
        state = combined(state, total, parts_ref[p, :rows], peak)


def with_header(body, *scalars):
    count, _, lanes = body.shape
    lines = [jnp.broadcast_to(x.reshape(count, 1, 1), (count, 1, lanes)) for x in scalars]
    lines.append(jnp.zeros((count, 8 - len(scalars), lanes), jnp.float32))
    return jnp.concatenate([body, *lines], axis=1)


def states_before(memory, totals, peaks):
    heads, dk, dv = memory.shape
    near = lax.axis_size(NEAR)
    far = lax.axis_size("far")
    rows = heads * dk // near
    per_head = near // heads
    sent = with_header(
        memory.reshape(near, rows, dv), jnp.repeat(totals, per_head), jnp.repeat(peaks, per_head)
    )
    got = traded(sent, NEAR)
    whole = pl.pallas_call(
        group_body,
        out_shape=jax.ShapeDtypeStruct(got.shape[1:], jnp.float32),
        compiler_params=pltpu.CompilerParams(vmem_limit_bytes=4 << 20),
        name="group_state",
    )(got)
    before = []
    for back in range(far - 1, 0, -1):
        before.append(lax.ppermute(whole, "far", [(i, i + back) for i in range(far - back)]))
    whole_spec = pl.BlockSpec(memory_space=pltpu.VMEM)
    states = pl.pallas_call(
        before_body,
        in_specs=[pl.BlockSpec(memory_space=pltpu.SMEM)] + [whole_spec] * far,
        out_specs=whole_spec,
        out_shape=jax.ShapeDtypeStruct(got.shape, jnp.float32),
        compiler_params=pltpu.CompilerParams(vmem_limit_bytes=4 << 20),
        name="states_before",
    )(lax.axis_index("far").reshape(1), got, *before)
    mine = traded(states, NEAR)
    return mine[:, :rows].reshape(heads, dk, dv), mine[::per_head, rows, 0]


def gathered_columns(matrix):
    own = jnp.transpose(matrix)
    far, near = lax.axis_size("far"), lax.axis_size("near")
    level = jnp.stack([own] + [shifted(own, "far", far - i) for i in range(1, far)])
    chips = far * near
    wide = []
    for k in (-1, 0, 1, 2):
        if k:
            wide.append(shifted(level, ("far", "near"), chips - k))
        else:
            wide.append(level)
    mine = jnp.stack(wide, axis=1).reshape(chips, *own.shape)
    other = shifted(mine, "core", 1)
    core = lax.axis_index("core")
    both = jnp.stack([jnp.where(core == 0, mine, other), jnp.where(core == 0, other, mine)], axis=1)
    both = both.reshape(chips, -1, own.shape[1])
    both = jnp.concatenate([both, both], axis=0)
    at = lax.axis_index(("far", "near"))
    start = jnp.where(at == 0, 1, chips + 1 - at)
    whole = lax.dynamic_slice_in_dim(both, start, chips, axis=0)
    return whole.reshape(-1, own.shape[1])


UNIT = 128
WIDE = 512


def expert_body(pieces, *refs):
    ins, (gate_hbm, up_hbm, down_hbm), refs = refs[:pieces], refs[pieces : pieces + 3], refs[pieces + 3 :]
    outs, refs = refs[:pieces], refs[pieces:]
    gate_ref, up_ref, down_ref, hidden_ref, gate_sem, up_sem, down_sem = refs
    units, columns, count = gate_ref.shape[0], down_ref.shape[0], ins[0].shape[0]

    def block(k, size):
        return pl.ds(pl.multiple_of(k * size, size), size)

    def gate_copy(k):
        return pltpu.make_async_copy(gate_hbm.at[:, block(k, UNIT)], gate_ref.at[k], gate_sem.at[k])

    def up_copy(k):
        return pltpu.make_async_copy(up_hbm.at[:, block(k, UNIT)], up_ref.at[k], up_sem.at[k])

    def down_copy(k):
        return pltpu.make_async_copy(down_hbm.at[:, block(k, WIDE)], down_ref.at[k], down_sem.at[k])

    def ask(k, _):
        gate_copy(k).start()
        up_copy(k).start()

    def hide(k, _):
        gate_copy(k).wait()
        up_copy(k).wait()
        both = jnp.concatenate([gate_ref[k], up_ref[k]], axis=1)
        rows = jnp.concatenate([ref[...] for ref in ins], axis=0)
        made = jnp.dot(rows, both, preferred_element_type=jnp.float32)
        gate, upward = made[:, :UNIT], made[:, UNIT:]
        hidden = gate / (1.0 + jnp.exp(-gate)) * upward
        hidden_ref[:, block(k, UNIT)] = hidden.astype(jnp.bfloat16)

    def show(k, _):
        down_copy(k).wait()
        made = jnp.dot(hidden_ref[...], down_ref[k], preferred_element_type=jnp.float32)
        made = made.astype(jnp.bfloat16)
        for n, out_ref in enumerate(outs):
            out_ref[:, block(k, WIDE)] = made[n * count : (n + 1) * count]

    lax.fori_loop(0, units, ask, None)
    lax.fori_loop(0, columns, lambda k, _: down_copy(k).start(), None)
    lax.fori_loop(0, units, hide, None)
    lax.fori_loop(0, columns, show, None)


def expert_parts(pieces, gate_w, up_w, down_w):
    count, width = pieces[0].shape
    inner = gate_w.shape[1]
    units, columns = inner // UNIT, width // WIDE
    whole = pl.BlockSpec(memory_space=pltpu.VMEM)
    stored = pl.BlockSpec(memory_space=pltpu.HBM)
    rows = jax.ShapeDtypeStruct((count, width), jnp.bfloat16)
    return pl.pallas_call(
        lambda *refs: expert_body(len(pieces), *refs),
        in_specs=[whole] * len(pieces) + [stored] * 3,
        out_specs=[whole] * len(pieces),
        out_shape=[rows] * len(pieces),
        scratch_shapes=[
            pltpu.VMEM((units, width, UNIT), jnp.bfloat16),
            pltpu.VMEM((units, width, UNIT), jnp.bfloat16),
            pltpu.VMEM((columns, inner, WIDE), jnp.bfloat16),
            pltpu.VMEM((len(pieces) * count, inner), jnp.bfloat16),
            pltpu.SemaphoreType.DMA((units,)),
            pltpu.SemaphoreType.DMA((units,)),
            pltpu.SemaphoreType.DMA((columns,)),
        ],
        compiler_params=pltpu.CompilerParams(vmem_limit_bytes=32 << 20),
        cost_estimate=pl.CostEstimate(
            flops=6 * len(pieces) * count * width * inner,
            bytes_accessed=6 * width * inner + 4 * len(pieces) * count * width,
            transcendentals=len(pieces) * count * inner,
        ),
        name="expert_parts",
    )(*pieces, gate_w, up_w, down_w)


def packed(by_slot, lines):
    slots, _, width = by_slot.shape
    if slots < lines:
        part = width * slots // lines
        rest = [by_slot[s, :, part:] for s in range(slots)]
        rest = jnp.concatenate(rest, axis=1)
        rest = rest.reshape(rest.shape[0], lines - slots, part).swapaxes(0, 1)
        by_slot = jnp.concatenate([by_slot[:, :, :part], rest], axis=0)
    return jnp.transpose(by_slot, (1, 0, 2))


def unpacked(messages, slots, width):
    lines, part = messages.shape[1:]
    by_line = jnp.transpose(messages, (1, 0, 2))
    if slots == lines:
        return by_line
    rest = by_line[slots:].swapaxes(0, 1).reshape(by_line.shape[1], -1)
    tail = width - part
    return jnp.stack(
        [
            jnp.concatenate([by_line[s], rest[:, s * tail : (s + 1) * tail]], axis=1)
            for s in range(slots)
        ]
    )


def through_experts(by_slot, weights):
    slots, peers, width = by_slot.shape
    rows = by_slot.reshape(slots * peers, width)
    size = lax.axis_size("tp")
    half = rows.shape[0] // 2
    left = shifted(rows, "tp", 1)
    right = shifted(rows, "tp", size - 1)
    across = [shifted(left[:half], "tp", 1), shifted(right[half:], "tp", size - 1)]
    left, right = lax.optimization_barrier((left, right))
    from_left, from_right = expert_parts((left, right), *weights)
    parts = [shifted(from_left, "tp", size - 1), shifted(from_right, "tp", 1)]
    across, _ = lax.optimization_barrier((jnp.concatenate(across, axis=0), from_right))
    (from_across,) = expert_parts((across,), *weights)
    parts.append(shifted(from_across, "tp", 2))
    rows, _ = lax.optimization_barrier((rows, from_across))
    parts.extend(expert_parts((rows,), *weights))
    made = sum(part.astype(jnp.float32) for part in parts).astype(jnp.bfloat16)
    return made.reshape(by_slot.shape), from_across


def shards(
    queries,
    head_key_rows,
    head_value_rows,
    input_gate_logit,
    forget_gate_preact,
    forget_log_offset,
    per_head_norm_gain,
    cell_output_matrix,
    layer_input_rows,
    expert_norm_gain,
    chosen_expert_index,
    chosen_expert_weight,
    expert_gate_matrix,
    expert_up_matrix,
    expert_down_matrix,
):
    count = queries.shape[0]
    heads = input_gate_logit.shape[0]
    queries3 = queries.reshape(count, heads, DK)
    keys3 = head_key_rows.reshape(count, heads, DK)
    values3 = head_value_rows.reshape(count, heads, DV)
    rows_at = lax.broadcasted_iota(jnp.int32, (count, count), 0)
    cols_at = lax.broadcasted_iota(jnp.int32, (count, count), 1)
    causal = cols_at <= rows_at

    log_retention = jax.nn.log_sigmoid(forget_gate_preact) + forget_log_offset
    running = jnp.dot(log_retention, (rows_at <= cols_at).astype(jnp.float32), precision=HIGHEST)
    totals = running[:, -1]
    term_log = totals[:, None] - running + input_gate_logit
    own_peak = jnp.max(term_log, axis=1)
    factors = jnp.transpose(jnp.exp(term_log - own_peak[:, None]))
    weighted = values3.astype(jnp.float32) * factors[:, :, None]
    own_memory = jnp.einsum(
        "shd,she->hde", keys3.astype(jnp.float32), weighted, precision=HIGHEST
    )

    memory_in, peak_in = states_before(own_memory, totals, own_peak)

    decay_log = jnp.where(
        causal[None],
        running[:, :, None] - running[:, None, :] + input_gate_logit[:, None, :],
        far_below,
    )
    carried_log = running + peak_in[:, None]
    peak = jnp.maximum(carried_log, jnp.max(decay_log, axis=2))
    qk_scale = DK ** (-0.5)
    scores = (
        jnp.einsum("thd,shd->hts", queries3, keys3, preferred_element_type=jnp.float32) * qk_scale
    )
    strength = scores * jnp.exp(decay_log - peak[:, :, None])
    carried = jnp.exp(carried_log - peak)
    from_memory = (
        jnp.einsum("thd,hde->the", queries3.astype(jnp.float32), memory_in, precision=HIGHEST)
        * qk_scale
    )
    within = jnp.einsum(
        "hts,she->the", strength.astype(jnp.bfloat16), values3, preferred_element_type=jnp.float32
    )
    result = within + jnp.transpose(carried)[:, :, None] * from_memory
    result = result * lax.rsqrt(jnp.mean(result * result, axis=2, keepdims=True) + norm_eps)
    result = result * per_head_norm_gain.astype(jnp.float32).reshape(heads, -1)
    mixed = result.reshape(count, -1).astype(jnp.bfloat16)

    partial_value = lax.dot_general(
        mixed,
        gathered_columns(cell_output_matrix),
        (((1,), (1,)), ((), ())),
        preferred_element_type=jnp.float32,
    ).astype(jnp.bfloat16)
    rows, width = layer_input_rows.shape
    tiles = traded(partial_value.reshape(lax.axis_size("tp"), rows, width), "tp")
    residual = layer_input_rows.astype(jnp.float32) + jnp.sum(tiles.astype(jnp.float32), axis=0)
    normed = residual * lax.rsqrt(jnp.mean(residual * residual, axis=1, keepdims=True) + norm_eps)
    normed = (normed * expert_norm_gain.astype(jnp.float32)).astype(jnp.bfloat16)

    experts = lax.axis_size(SP)
    slots = (4 * rows + experts - 1) // experts
    expert_at = jnp.arange(experts, dtype=jnp.int32)[None, :]
    named = [
        (chosen_expert_index[:, k : k + 1] == expert_at).astype(jnp.bfloat16) for k in range(2)
    ]
    below = (
        lax.broadcasted_iota(jnp.int32, (rows, rows), 1)
        < lax.broadcasted_iota(jnp.int32, (rows, rows), 0)
    ).astype(jnp.bfloat16)
    ahead = [jnp.dot(below, n, preferred_element_type=jnp.float32) for n in named]
    first = jnp.sum(named[0].astype(jnp.float32), axis=0, keepdims=True)
    ahead[1] = ahead[1] + first
    picks = []
    for k in range(2):
        place = jnp.sum(named[k].astype(jnp.float32) * ahead[k], axis=1, keepdims=True)
        slot = place.astype(jnp.int32) * experts + chosen_expert_index[:, k : k + 1]
        target = lax.broadcasted_iota(jnp.int32, (rows, experts * slots), 1)
        picks.append((slot == target).astype(jnp.bfloat16))
    outgoing = lax.dot_general(
        picks[0] + picks[1],
        normed,
        (((0,), (0,)), ((), ())),
        preferred_element_type=jnp.float32,
    ).astype(jnp.bfloat16)

    weights = tuple(pltpu.with_memory_space_constraint(w[0], pltpu.HBM) for w in (expert_gate_matrix, expert_up_matrix, expert_down_matrix))
    early, lines = slots // 2, (slots + 1) // 2
    by_slot = outgoing.reshape(slots, experts, width)
    got_a = traded(packed(by_slot[:early], lines), SP)
    got_b = traded(packed(by_slot[early:], lines), SP)
    made_a, last = through_experts(unpacked(got_a, early, width), weights)
    got_b, _ = lax.optimization_barrier((got_b, last))
    back_a = traded(packed(made_a, lines), SP)
    made_b, _ = through_experts(unpacked(got_b, slots - early, width), weights)
    back_b = traded(packed(made_b, lines), SP)

    out = residual
    cut = early * experts
    out_a = unpacked(back_a, early, width).reshape(cut, width)
    out_b = unpacked(back_b, slots - early, width).reshape(-1, width)
    for k in range(2):
        picked = jnp.dot(picks[k][:, :cut], out_a, preferred_element_type=jnp.float32)
        out = out + chosen_expert_weight[:, k : k + 1] * picked
    for k in range(2):
        picked = jnp.dot(picks[k][:, cut:], out_b, preferred_element_type=jnp.float32)
        out = out + chosen_expert_weight[:, k : k + 1] * picked
    return out.astype(jnp.bfloat16)


def solution(mesh):
    sp = mesh.shape["sp"]
    torus = Mesh(
        mesh.devices.reshape(mesh.shape["grp"], sp // 8, 4, 2, mesh.shape["tp"]), GRP_SP_TP
    )
    return jax.shard_map(
        shards,
        mesh=torus,
        in_specs=(
            P(GRP_SP, "tp"),
            P(GRP_SP, "tp"),
            P(GRP_SP, "tp"),
            P("tp", GRP_SP),
            P("tp", GRP_SP),
            P("tp", GRP_SP),
            P("tp"),
            P("tp", SP),
            P(GRP_SP_TP, None),
            P(),
            P(GRP_SP_TP, None),
            P(GRP_SP_TP, None),
            P(SP, None, "tp"),
            P(SP, None, "tp"),
            P(SP, "tp", None),
        ),
        out_specs=P(GRP_SP_TP, None),
        check_vma=False,
    )
```
